32 devices in a mesh: sp: 16 (over z, y, x), tp: 2 (over core).
Axes of the slice: x: 2, y: 2, z: 4, core: 2. Of those that a mesh axis runs over, the one named last changes fastest.
Arguments:
- queries: bfloat16 [4096, 512], P('sp', 'tp'), may hold values from -6 to 6
- keys: bfloat16 [4096, 512], P('sp', 'tp'), may hold values from -6 to 6
- values: bfloat16 [4096, 512], P('sp', 'tp'), may hold values from -6 to 6
- gains: float32 [2, 128], replicated, may hold values from 0.1 to 1.9
- bias_table: float32 [192, 4], P(None, 'tp'), may hold values from -6 to 270
- d_out: bfloat16 [4096, 512], P('sp', 'tp'), may hold values from -32 to 32
Outputs:
- d_queries: bfloat16 [4096, 512], P('sp', 'tp')
- d_keys: bfloat16 [4096, 512], P('sp', 'tp')
- d_values: bfloat16 [4096, 512], P('sp', 'tp')
- d_table: float32 [192, 4], P(None, 'tp')
- d_gains: float32 [2, 128], replicated
The draws below stay inside these ranges and needn't reach their ends.
All inputs are finite; a program needn't handle non-finite values.
Results may differ from the reference program's by a relative error of at most 0.008.
Values may be sent and summed in bfloat16 or wider, within the bound.
A program may use at most 64 MiB of HBM per device.

```python
import jax
import jax.numpy as jnp
from jax import lax

HEADS = 4
HEAD_DIM = 128
SEG = 64
LEFT = 4
MAX_REL = 128
TOKENS = 4096


def draw_bias_table(key, part):
    entries = MAX_REL + SEG
    rough = jnp.clip(jax.random.normal(key, (entries, HEADS), jnp.float32), -6.0, 6.0)
    return rough.astype(jnp.float32)


def draw_d_out(key, part):
    width = HEADS * HEAD_DIM
    position = jnp.arange(TOKENS).astype(jnp.float32)[:, None] / TOKENS
    spread = 10.0 ** (jax.random.uniform(jax.random.fold_in(key, 1), (TOKENS, 1), jnp.float32) - 1.0)
    base = jnp.clip(jax.random.normal(jax.random.fold_in(key, 2), (TOKENS, width), jnp.float32), -6.0, 6.0)
    rise = 3.0 ** position
    return (base * spread * rise).astype(jnp.bfloat16)


def shard_levels(own_key, dims, shards, smallest, high):
    gain = 1.0
    for axis_at, shards_of in shards:
        heights = jax.random.uniform(jax.random.fold_in(jax.random.fold_in(own_key, 6), axis_at), (shards_of,), jnp.float32, smallest / len(shards), high / len(shards))
        gain = gain * jnp.repeat(jnp.exp(heights), dims[axis_at] // shards_of).reshape((-1,) + (1,) * (len(dims) - 1 - axis_at))
    return gain


def centred(own_key, shape, scale, bound, cuts=(), held_as=jnp.bfloat16):
    values = scale * jax.random.normal(own_key, shape, jnp.float32)
    if cuts:
        values = values * shard_levels(own_key, shape, cuts, -0.22, 0.18)
    return jnp.clip(values, -bound, bound).astype(held_as)


def setup_inputs(seed: int = 0) -> dict:
    streams_of = jax.random.split(jax.random.key(seed), 7)
    return {
        "queries": centred(streams_of[0], (TOKENS, HEADS * HEAD_DIM), 1.0, 6.0, ((0, 16), (1, 2))),
        "keys": centred(streams_of[1], (TOKENS, HEADS * HEAD_DIM), 1.0, 6.0, ((0, 16), (1, 2))),
        "values": centred(streams_of[2], (TOKENS, HEADS * HEAD_DIM), 1.0, 6.0, ((0, 16), (1, 2))),
        "gains": jnp.clip(1.0 + 0.18 * jax.random.normal(streams_of[3], (2, HEAD_DIM), jnp.float32), 0.1, 1.9),
        "bias_table": draw_bias_table(jax.random.fold_in(streams_of[6], 71), 0),
        "d_out": draw_d_out(jax.random.fold_in(streams_of[6], 71), 0),
    }


EPSILON = 1e-06

def unit_rows(row_block):
    widened = row_block.astype(jnp.float32).reshape(row_block.shape[0], HEADS, HEAD_DIM)
    inv_rms = lax.rsqrt(lax.optimization_barrier(jnp.mean(widened * widened, axis=-1, keepdims=True)) + EPSILON)
    return (widened * inv_rms, inv_rms)

def rows_back(d_normed, row_block, gain_vec):
    unit_part, inv_rms = unit_rows(row_block)
    d_unit = d_normed * gain_vec
    d_rows = inv_rms * (d_unit - unit_part * lax.optimization_barrier(jnp.mean(d_unit * unit_part, axis=-1, keepdims=True)))
    return (d_rows.reshape(row_block.shape[0], -1).astype(jnp.bfloat16), lax.optimization_barrier(jnp.sum(d_normed * unit_part, axis=(0, 1))))

def lowered(array_in):
    return lax.optimization_barrier(array_in.astype(jnp.bfloat16)).astype(jnp.float32)

def reference(queries, keys, values, gains, bias_table, d_out):
    tail_rows = LEFT * SEG
    blocks = TOKENS // tail_rows
    factor = HEAD_DIM ** (-0.5)
    q_unit, _ = unit_rows(queries)
    q_norm = (q_unit * gains[0]).astype(jnp.bfloat16)
    k_unit, _ = unit_rows(keys)
    k_norm = (k_unit * gains[1]).astype(jnp.bfloat16)
    leading = jnp.zeros((tail_rows, HEADS, HEAD_DIM), jnp.bfloat16)
    k_all = jnp.concatenate([leading, k_norm])
    v_all = jnp.concatenate([leading, values.reshape(TOKENS, HEADS, HEAD_DIM)])
    q_blocks = q_norm.reshape(blocks, tail_rows, HEADS, HEAD_DIM)
    do_blocks = d_out.reshape(blocks, tail_rows, HEADS, HEAD_DIM)
    query_idx = jnp.arange(tail_rows, dtype=jnp.int32)[:, None]
    key_idx = jnp.arange(2 * tail_rows, dtype=jnp.int32)[None, :]
    rel_index = (jnp.clip(query_idx + tail_rows - key_idx, -(SEG - 1), MAX_REL) + SEG - 1).astype(jnp.int32)
    bias_tiles = jnp.transpose(bias_table[rel_index], (2, 0, 1))
    flat_index = rel_index.reshape(-1)

    def advance(state, entry):
        pend_k, pend_v, table_sum = state
        number, q_block, do_block = entry
        start = number * tail_rows
        k_ext = lax.dynamic_slice_in_dim(k_all, start, 2 * tail_rows, 0).astype(jnp.float32)
        v_ext = lax.dynamic_slice_in_dim(v_all, start, 2 * tail_rows, 0).astype(jnp.float32)
        query_seg = (start + query_idx) // SEG
        key_pos = start - tail_rows + key_idx
        key_seg = key_pos // SEG
        key_valid = (key_pos >= 0) & (key_seg >= query_seg - LEFT) & (key_seg <= query_seg)
        q_float = q_block.astype(jnp.float32)
        do_float = do_block.astype(jnp.float32)
        scores = jnp.einsum('ihd,jhd->hij', q_float, k_ext) * factor + bias_tiles
        scores = jnp.where(key_valid[None], scores, -jnp.inf)
        row_max = lax.optimization_barrier(jnp.max(scores, axis=-1, keepdims=True))
        log_total = row_max + jnp.log(lax.optimization_barrier(jnp.sum(jnp.exp(scores - row_max), axis=-1, keepdims=True)))
        prob = jnp.exp(scores - log_total)
        d_prob = jnp.einsum('ihd,jhd->hij', do_float, v_ext)
        row_delta = lax.optimization_barrier(jnp.sum(prob * d_prob, axis=-1, keepdims=True))
        d_score = prob * (d_prob - row_delta)
        prob_low = lowered(prob)
        d_low = lowered(d_score)
        grad_v = jnp.einsum('hij,ihd->jhd', prob_low, do_float)
        grad_k = jnp.einsum('hij,ihd->jhd', d_low, q_float) * factor
        grad_q = jnp.einsum('hij,jhd->ihd', d_low, k_ext) * factor
        table_part = jax.ops.segment_sum(jnp.transpose(d_score, (1, 2, 0)).reshape(-1, HEADS), flat_index, num_segments=MAX_REL + SEG)
        emitted = (pend_k + grad_k[:tail_rows], pend_v + grad_v[:tail_rows], grad_q)
        return ((grad_k[tail_rows:], grad_v[tail_rows:], table_sum + table_part), emitted)
    zero_rows = jnp.zeros((tail_rows, HEADS, HEAD_DIM), jnp.float32)
    initial = (zero_rows, zero_rows, jnp.zeros((MAX_REL + SEG, HEADS), jnp.float32))
    numbers = jnp.arange(blocks, dtype=jnp.int32)
    (last_k, last_v, d_table), (ys_k, ys_v, ys_q) = lax.scan(advance, initial, (numbers, q_blocks, do_blocks))
    d_kn = jnp.concatenate([ys_k[1:].reshape(-1, HEADS, HEAD_DIM), last_k])
    d_vn = jnp.concatenate([ys_v[1:].reshape(-1, HEADS, HEAD_DIM), last_v])
    d_qn = ys_q.reshape(TOKENS, HEADS, HEAD_DIM)
    d_queries, gain_q = rows_back(d_qn, queries, gains[0])
    d_keys, gain_k = rows_back(d_kn, keys, gains[1])
    d_values = d_vn.reshape(TOKENS, -1).astype(jnp.bfloat16)
    return (d_queries, d_keys, d_values, d_table, jnp.stack([gain_q, gain_k]))
```

```python
import functools

import jax
import jax.numpy as jnp
from jax import lax
from jax.experimental import pallas as pl
from jax.experimental.pallas import tpu as pltpu
from jax.sharding import PartitionSpec as P

HEAD_DIM = 128
SEG = 64
LEFT = 4
MAX_REL = 128
EPSILON = 1e-06
NEG = -1e30
LOG2E = 1.4426950408889634
MESH = pl.DeviceIdType.MESH
F32 = jnp.float32
BF16 = jnp.bfloat16


def dot(a, b, contract):
    return lax.dot_general(a, b, ((contract[:1], contract[1:]), ((), ())), preferred_element_type=F32)


def unit_of(block):
    wide = block.astype(F32)
    rms = lax.rsqrt(jnp.mean(wide * wide, axis=-1, keepdims=True) + EPSILON)
    return wide * rms, rms


def diagonals(tile, lead):
    rows, lanes = tile.shape
    total = None
    for start in range(0, rows, 8):
        turned = pltpu.roll(tile[start : start + 8], (lead - start) % lanes, 1)
        total = turned if total is None else total + turned
    sublane = lax.broadcasted_iota(jnp.int32, total.shape, 0)
    line = jnp.where(sublane == 0, total, 0.0)
    for i in range(1, 8):
        line = line + jnp.where(sublane == i, pltpu.roll(total, lanes - i, 1), 0.0)
    return jnp.sum(line, axis=0, keepdims=True)


def kernel(
    n_sp, n_tp,
    q_hbm, k_hbm, v_hbm, do_hbm, g_hbm, t_hbm,
    dq_ref, dk_ref, dv_ref, dt_ref, dg_ref,
    q_ref, k_ref, v_ref, do_ref, g_ref, t_ref, k_raw, v_prev, kn, qn, q_unit, q_rms, k_unit, k_rms,
    tiles, e_own, dp_own, dk_acc, dv_acc, dk_out, dv_out, dk_in, dv_in, one_src, two, line_src, lines,
    load_sem, send_sem, recv_sem, red_sem, hand_sem,
):
    heads, rows, _ = q_ref.shape
    half = rows // 2
    entries = t_ref.shape[1]
    lead = SEG - 1
    factor = HEAD_DIM ** (-0.5)
    scale = factor * LOG2E
    sp, tp = lax.axis_index("sp"), lax.axis_index("tp")
    has_prev, has_next = sp > 0, sp < n_sp - 1
    nxt, prv = sp + 1, sp - 1

    def load(src, dst, slot):
        return pltpu.make_async_copy(src, dst, load_sem.at[slot])

    def by_head(src, dst, slot):
        return [load(src.at[:, pl.ds(h * HEAD_DIM, HEAD_DIM)], dst.at[h], slot + h) for h in range(heads)]

    load_k = by_head(k_hbm, k_ref, 0)
    load_v = by_head(v_hbm, v_ref, heads)
    load_small = [load(t_hbm, t_ref, 4 * heads), load(g_hbm, g_ref, 4 * heads + 1)]
    load_q = by_head(q_hbm, q_ref, 2 * heads)
    load_do = by_head(do_hbm, do_ref, 3 * heads)
    for copy in load_k + load_v + load_small + load_q + load_do:
        copy.start()

    def signal(sem, at, core):
        pl.semaphore_signal(sem, inc=1, device_id=(at, core), device_id_type=MESH)

    def around(sem, radius):
        @pl.when(sp >= radius)
        def _():
            signal(sem, sp - radius, tp)

        @pl.when(sp < n_sp - radius)
        def _():
            signal(sem, sp + radius, tp)

    def count_around(radius):
        return jnp.where(sp >= radius, 1, 0) + jnp.where(sp < n_sp - radius, 1, 0)

    barrier = pltpu.get_barrier_semaphore()
    around(barrier, 1)
    for other in range(1, n_tp):
        signal(barrier, sp, lax.rem(tp + other, n_tp))
    pl.semaphore_wait(barrier, count_around(1) + n_tp - 1)

    rounds = []
    while 2 ** len(rounds) < n_sp:
        rounds.append(2 ** len(rounds))

    def say(step):
        around(hand_sem.at[step], rounds[step])

    def hear(step):
        pl.semaphore_wait(hand_sem.at[step], count_around(rounds[step]))

    def send(slot, src, dst, to):
        return pltpu.make_async_remote_copy(
            src_ref=src, dst_ref=dst, send_sem=send_sem.at[slot], recv_sem=recv_sem.at[slot],
            device_id=(to, tp), device_id_type=MESH,
        )

    k_next = [send(4 * h, k_ref.at[h], k_raw.at[h], nxt) for h in range(heads)]
    v_next = [send(4 * h + 1, v_ref.at[h], v_prev.at[h], nxt) for h in range(heads)]
    dv_back = [send(4 * h + 2, dv_out.at[h], dv_in.at[h], prv) for h in range(heads)]
    dk_back = [send(4 * h + 3, dk_out.at[h], dk_in.at[h], prv) for h in range(heads)]

    def start(gate, copies):
        @pl.when(gate)
        def _():
            for copy in copies:
                copy.start()

    for copy in load_k + load_v:
        copy.wait()
    for h in range(heads):
        start(has_next, [k_next[h], v_next[h]])
    say(0)
    for copy in load_small:
        copy.wait()

    @pl.when(jnp.logical_not(has_prev))
    def _():
        kn[:, 0:rows, :] = jnp.zeros((heads, rows, HEAD_DIM), BF16)
        v_prev[...] = jnp.zeros((heads, rows, HEAD_DIM), BF16)

    g0, g1 = g_ref[0:1, :], g_ref[1:2, :]
    low, high = slice(0, half), slice(half, rows)
    row = lax.broadcasted_iota(jnp.int32, (half, half), 0)
    col = lax.broadcasted_iota(jnp.int32, (half, half), 1)
    upper = col >= row
    absent = jnp.where(has_prev, 0.0, NEG)

    table = jnp.concatenate([t_ref[...], jnp.zeros((heads, 2 * half - entries), F32)], axis=1)
    table = pltpu.roll(table, 2 * half - lead, 1)
    for h in range(heads):
        def skew(line):
            return pltpu.roll(jnp.broadcast_to(line, (half, half)), 0, 1, stride=1, stride_axis=0)

        near = skew(table[h : h + 1, 0:half])
        ahead = skew(table[h : h + 1, half:])
        far = jnp.broadcast_to(table[h : h + 1, half : half + 1], (half, half))
        same = jnp.where(upper, near, ahead)
        same = jnp.where((row >= SEG) & (col < SEG), NEG, same)
        before = jnp.where(upper, far, near)
        distant = jnp.where((row < SEG) & (col >= SEG), NEG, far)
        top_own = jnp.max(same, axis=0, keepdims=True)
        top = jnp.maximum(top_own, jnp.max(before, axis=0, keepdims=True))
        first_top = jnp.where(has_prev, top, top_own)
        tiles[h, 0] = (same - first_top) * LOG2E
        tiles[h, 1] = (before - top) * LOG2E
        tiles[h, 2] = (same - top) * LOG2E
        tiles[h, 3] = (distant - top) * LOG2E + absent
        tiles[h, 4] = (before - top) * LOG2E + absent

    for h in range(heads):
        unit, rms = unit_of(k_ref[h])
        k_unit[h] = unit
        k_rms[h] = rms
        kn[h, rows:, :] = (unit * g1).astype(BF16)
    hear(0)
    say(1)
    for copy in load_q + load_do:
        copy.wait()

    sums = []
    for h in range(heads):
        unit, rms = unit_of(q_ref[h])
        q_unit[h] = unit
        q_rms[h] = rms
        qn[h] = (unit * g0).astype(BF16)
        s0 = dot(kn[h, rows : rows + half, :], qn[h], (1, 1)) * scale
        s1 = dot(kn[h, rows + half :, :], qn[h, high, :], (1, 1)) * scale
        e0 = jnp.exp2(s0[:, low] + tiles[h, 0])
        e1 = jnp.exp2(s0[:, high] + tiles[h, 1])
        e2 = jnp.exp2(s1 + tiles[h, 2])
        e_own[h, 0], e_own[h, 1], e_own[h, 2] = e0, e1, e2
        p0 = dot(v_ref[h, low, :], do_ref[h], (1, 1))
        dp_own[h, 0], dp_own[h, 1] = p0[:, low], p0[:, high]
        dp_own[h, 2] = dot(v_ref[h, high, :], do_ref[h, high, :], (1, 1))
        sums.append((
            jnp.sum(e0, axis=0, keepdims=True),
            jnp.sum(e1, axis=0, keepdims=True) + jnp.sum(e2, axis=0, keepdims=True),
        ))
        if h + 1 < len(rounds):
            hear(h + 1)
        if h + 2 < len(rounds):
            say(h + 2)
    for step in range(heads + 1, len(rounds)):
        hear(step)
        if step + 1 < len(rounds):
            say(step + 1)

    packed = []
    mass = jnp.zeros((1, HEAD_DIM), F32)
    for h in range(heads):
        @pl.when(has_prev)
        def _():
            k_next[h].wait_recv()
            kn[h, 0:rows, :] = (unit_of(k_raw[h])[0] * g1).astype(BF16)

        s0 = dot(kn[h, low, :], qn[h, low, :], (1, 1)) * scale
        s1 = dot(kn[h, high, :], qn[h], (1, 1)) * scale
        x0 = jnp.exp2(s0 + tiles[h, 3])
        x1 = jnp.exp2(s1[:, low] + tiles[h, 4])
        x2 = jnp.exp2(s1[:, high] + tiles[h, 3])
        r0 = 1.0 / (sums[h][0] + jnp.sum(x0 + x1, axis=0, keepdims=True))
        r1 = 1.0 / (sums[h][1] + jnp.sum(x2, axis=0, keepdims=True))
        x0, x1, x2 = x0 * r0, x1 * r0, x2 * r1
        e0, e1, e2 = e_own[h, 0] * r0, e_own[h, 1] * r1, e_own[h, 2] * r1
        d_o = do_ref[h]
        dv_out[h, low, :] = dot(x0.astype(BF16), d_o[low], (1, 0)).astype(BF16)
        dv_out[h, high, :] = dot(jnp.concatenate([x1, x2], axis=1).astype(BF16), d_o, (1, 0)).astype(BF16)
        dv_acc[h, low, :] = dot(jnp.concatenate([e0, e1], axis=1).astype(BF16), d_o, (1, 0))
        dv_acc[h, high, :] = dot(e2.astype(BF16), d_o[high], (1, 0))
        if h < heads - 1:
            start(has_prev, [dv_back[h]])
        own0 = jnp.sum(e0 * dp_own[h, 0], axis=0, keepdims=True)
        own1 = jnp.sum(e1 * dp_own[h, 1] + e2 * dp_own[h, 2], axis=0, keepdims=True)

        @pl.when(has_prev)
        def _():
            v_next[h].wait_recv()

        p0 = dot(v_prev[h, low, :], d_o[low], (1, 1))
        p1 = dot(v_prev[h, high, :], d_o, (1, 1))
        delta0 = own0 + jnp.sum(x0 * p0 + x1 * p1[:, low], axis=0, keepdims=True)
        delta1 = own1 + jnp.sum(x2 * p1[:, high], axis=0, keepdims=True)
        x0, x1, x2 = x0 * (p0 - delta0), x1 * (p1[:, low] - delta0), x2 * (p1[:, high] - delta1)
        e0, e1, e2 = e0 * (dp_own[h, 0] - delta0), e1 * (dp_own[h, 1] - delta1), e2 * (dp_own[h, 2] - delta1)
        blocks = [
            x0.astype(BF16),
            jnp.concatenate([x1, x2], axis=1).astype(BF16),
            jnp.concatenate([e0, e1], axis=1).astype(BF16),
            e2.astype(BF16),
        ]
        spans = [low, slice(0, rows), slice(0, rows), high]
        d_k = [dot(block, qn[h, span, :], (1, 0)) for block, span in zip(blocks, spans)]
        product = None
        for i, part in enumerate(d_k):
            term = part * kn[h, i * half : (i + 1) * half, :].astype(F32)
            product = term if product is None else product + term
        mass = mass + jnp.sum(product, axis=0, keepdims=True)
        same, before = e0 + e2, x1 + e1
        line_p = diagonals(jnp.where(upper, same, before), lead)
        line_n = diagonals(jnp.where(upper, 0.0, same), lead)
        lane = lax.broadcasted_iota(jnp.int32, line_p.shape, 1)
        rest = -(jnp.sum(line_p, axis=1, keepdims=True) + jnp.sum(line_n, axis=1, keepdims=True))
        packed.append(jnp.where(lane < lead, line_n, line_p))
        packed.append(jnp.where(lane < lead, line_p, jnp.where(lane == lead, rest, 0.0)))
        dk_out[h, low, :] = d_k[0].astype(BF16)
        dk_out[h, high, :] = d_k[1].astype(BF16)
        dk_acc[h, low, :] = d_k[2]
        dk_acc[h, high, :] = d_k[3]
        if h < heads - 1:
            start(has_prev, [dk_back[h]])
        else:
            mass = mass * factor
            line_src[...] = mass
            one_src[...] = jnp.concatenate(
                packed + [mass, jnp.zeros((8 - 1 - len(packed), HEAD_DIM), F32)], axis=0
            )
            two[sp] = one_src[...]

            def spread(i):
                at = jnp.where(i >= sp, i + 1, i)
                pltpu.make_async_remote_copy(
                    src_ref=one_src, dst_ref=two.at[sp], send_sem=red_sem.at[0], recv_sem=red_sem.at[1],
                    device_id=(at, tp), device_id_type=MESH,
                ).start()

            def spread_line(at):
                for other in range(1, n_tp):
                    pltpu.make_async_remote_copy(
                        src_ref=line_src, dst_ref=lines.at[other - 1, sp], send_sem=red_sem.at[2],
                        recv_sem=red_sem.at[3], device_id=(at, lax.rem(tp + other, n_tp)), device_id_type=MESH,
                    ).start()

            if n_sp <= 32:
                for i in range(n_sp - 1):
                    spread(i)
                    spread_line(i)
                spread_line(n_sp - 1)
            else:
                @pl.loop(0, n_sp - 1)
                def _(i):
                    spread(i)

                @pl.loop(0, n_sp)
                def _(i):
                    spread_line(i)

            start(has_prev, [dv_back[h], dk_back[h]])
        for i, part in enumerate([
            dot(jnp.concatenate([blocks[0], blocks[1][:, low], blocks[2][:, low]], axis=0), kn[h, 0 : 3 * half, :], (0, 0)),
            dot(jnp.concatenate([blocks[1][:, high], blocks[2][:, high], blocks[3]], axis=0), kn[h, half:, :], (0, 0)),
        ]):
            span = slice(i * half, (i + 1) * half)
            grad = part * factor * g0
            unit = q_unit[h, span, :]
            out = q_rms[h, span, :] * (grad - unit * jnp.mean(grad * unit, axis=-1, keepdims=True))
            dq_ref[span, h * HEAD_DIM : (h + 1) * HEAD_DIM] = out.astype(BF16)

    for h in range(heads):
        across = slice(h * HEAD_DIM, (h + 1) * HEAD_DIM)

        @pl.when(has_next)
        def _():
            dv_back[h].wait_recv()
            dk_back[h].wait_recv()
            dv_acc[h] += dv_in[h].astype(F32)
            dk_acc[h] += dk_in[h].astype(F32)

        dv_ref[:, across] = dv_acc[h].astype(BF16)
        unit = k_unit[h]
        grad = dk_acc[h] * factor * g1
        out = k_rms[h] * (grad - unit * jnp.mean(grad * unit, axis=-1, keepdims=True))
        dk_ref[:, across] = out.astype(BF16)

    inverse = 1.0 / g_ref[...]
    peers = two.at[pl.ds(0, n_sp - 1)]
    pltpu.make_async_copy(peers, peers, red_sem.at[1]).wait()
    pltpu.make_async_copy(lines, lines, red_sem.at[3]).wait()
    whole = jnp.sum(two[...], axis=0)
    for h in range(heads):
        dt_ref[h : h + 1, 0:half] = whole[2 * h : 2 * h + 1]
        dt_ref[h : h + 1, half:] = whole[2 * h + 1 : 2 * h + 2, 0 : entries - half]
    mass = whole[2 * heads : 2 * heads + 1] + jnp.sum(lines[...], axis=(0, 1))
    dg_ref[...] = mass * inverse

    pltpu.make_async_copy(peers, peers, red_sem.at[0]).wait()
    pltpu.make_async_copy(lines, lines, red_sem.at[2]).wait()

    @pl.when(has_next)
    def _():
        for copy in k_next + v_next:
            copy.wait_send()

    @pl.when(has_prev)
    def _():
        for copy in dv_back + dk_back:
            copy.wait_send()


def emit(*refs):
    sem = refs[-1]
    count = len(refs) // 2
    copies = [pltpu.make_async_copy(refs[i], refs[count + i], sem.at[i]) for i in range(count)]
    for copy in copies:
        copy.start()
    for copy in copies:
        copy.wait()


def solution(mesh):
    n_sp, n_tp = mesh.shape["sp"], mesh.shape["tp"]

    def local(queries, keys, values, gains, bias_table, d_out):
        rows, width = queries.shape
        heads = width // HEAD_DIM
        half = rows // 2
        assert n_sp > 1 and rows == LEFT * SEG and half == MAX_REL == HEAD_DIM and 2 * heads + 1 <= 8
        act = jax.ShapeDtypeStruct((rows, width), BF16)
        vmem = pl.BlockSpec(memory_space=pltpu.VMEM)
        shapes = (
            act, act, act,
            jax.ShapeDtypeStruct(bias_table.shape[::-1], F32),
            jax.ShapeDtypeStruct(gains.shape, F32),
        )
        low = pltpu.VMEM((heads, rows, HEAD_DIM), BF16)
        wide = pltpu.VMEM((heads, rows, HEAD_DIM), F32)
        thin = pltpu.VMEM((heads, rows, 1), F32)
        parts = pl.pallas_call(
            functools.partial(kernel, n_sp, n_tp),
            out_shape=shapes,
            in_specs=[pl.BlockSpec(memory_space=pltpu.HBM)] * 6,
            out_specs=(vmem,) * 5,
            scratch_shapes=[
                low, low, low, low,
                pltpu.VMEM(gains.shape, F32),
                pltpu.VMEM(bias_table.shape[::-1], F32),
                low, low,
                pltpu.VMEM((heads, 2 * rows, HEAD_DIM), BF16),
                low,
                wide, thin, wide, thin,
                pltpu.VMEM((heads, 5, half, half), F32),
                pltpu.VMEM((heads, 3, half, half), F32),
                pltpu.VMEM((heads, 3, half, half), F32),
                wide, wide,
                low, low, low, low,
                pltpu.VMEM((8, HEAD_DIM), F32),
                pltpu.VMEM((n_sp, 8, HEAD_DIM), F32),
                pltpu.VMEM((1, HEAD_DIM), F32),
                pltpu.VMEM((n_tp - 1, n_sp, 1, HEAD_DIM), F32),
                pltpu.SemaphoreType.DMA((4 * heads + 2,)),
                pltpu.SemaphoreType.DMA((4 * heads,)),
                pltpu.SemaphoreType.DMA((4 * heads,)),
                pltpu.SemaphoreType.DMA((4,)),
                pltpu.SemaphoreType.REGULAR((max(1, (n_sp - 1).bit_length()),)),
            ],
            compiler_params=pltpu.CompilerParams(
                collective_id=0, has_side_effects=True, vmem_limit_bytes=24 * 1024 * 1024
            ),
        )(*(
            pltpu.with_memory_space_constraint(x, pltpu.HBM)
            for x in (queries, keys, values, d_out, gains, bias_table.T)
        ))
        d_q, d_k, d_v, d_table, d_gains = pl.pallas_call(
            emit,
            out_shape=shapes,
            in_specs=[vmem] * 5,
            out_specs=(pl.BlockSpec(memory_space=pltpu.HBM),) * 5,
            scratch_shapes=[pltpu.SemaphoreType.DMA((5,))],
            compiler_params=pltpu.CompilerParams(vmem_limit_bytes=8 * 1024 * 1024),
        )(*parts)
        return d_q, d_k, d_v, d_table.T, d_gains

    in_specs = (P("sp", "tp"), P("sp", "tp"), P("sp", "tp"), P(), P(None, "tp"), P("sp", "tp"))
    out_specs = (P("sp", "tp"), P("sp", "tp"), P("sp", "tp"), P(None, "tp"), P())
    return jax.shard_map(local, mesh=mesh, in_specs=in_specs, out_specs=out_specs, check_vma=False)
```

```python
import functools

import jax
import jax.numpy as jnp
from jax import lax
from jax.experimental import pallas as pl
from jax.experimental.pallas import tpu as pltpu
from jax.sharding import PartitionSpec as P

HEAD_DIM = 128
SEG = 64
LEFT = 4
MAX_REL = 128
EPSILON = 1e-06
NEG = -1e30
LOG2E = 1.4426950408889634
MESH = pl.DeviceIdType.MESH
F32 = jnp.float32
BF16 = jnp.bfloat16


def dot(a, b, contract):
    return lax.dot_general(a, b, ((contract[:1], contract[1:]), ((), ())), preferred_element_type=F32)


def unit_of(block):
    wide = block.astype(F32)
    rms = lax.rsqrt(jnp.mean(wide * wide, axis=-1, keepdims=True) + EPSILON)
    return wide * rms, rms


def diagonals(tile, lead):
    rows, lanes = tile.shape
    total = None
    for start in range(0, rows, 8):
        turned = pltpu.roll(tile[start : start + 8], (lead - start) % lanes, 1)
        total = turned if total is None else total + turned
    sublane = lax.broadcasted_iota(jnp.int32, total.shape, 0)
    line = jnp.where(sublane == 0, total, 0.0)
    for i in range(1, 8):
        line = line + jnp.where(sublane == i, pltpu.roll(total, lanes - i, 1), 0.0)
    return jnp.sum(line, axis=0, keepdims=True)


def kernel(
    n_sp, n_tp,
    q_hbm, k_hbm, v_hbm, do_hbm, g_hbm, t_hbm,
    dq_ref, dk_ref, dv_ref, dt_ref, dg_ref,
    q_ref, k_ref, v_ref, do_ref, g_ref, t_ref, k_raw, v_prev, kn, qn, q_unit, q_rms, k_unit, k_rms,
    tiles, e_own, dp_own, dk_acc, dv_acc, dk_out, dv_out, dk_in, dv_in, one_src, two, line_src, lines,
    load_sem, send_sem, recv_sem, red_sem, hand_sem,
):
    heads, rows, _ = q_ref.shape
    half = rows // 2
    entries = t_ref.shape[1]
    lead = SEG - 1
    factor = HEAD_DIM ** (-0.5)
    scale = factor * LOG2E
    sp, tp = lax.axis_index("sp"), lax.axis_index("tp")
    has_prev, has_next = sp > 0, sp < n_sp - 1
    nxt, prv = sp + 1, sp - 1

    def load(src, dst, slot):
        return pltpu.make_async_copy(src, dst, load_sem.at[slot])

    def by_head(src, dst, slot):
        return [load(src.at[:, pl.ds(h * HEAD_DIM, HEAD_DIM)], dst.at[h], slot + h) for h in range(heads)]

    load_k = by_head(k_hbm, k_ref, 0)
    load_v = by_head(v_hbm, v_ref, heads)
    load_small = [load(t_hbm, t_ref, 4 * heads), load(g_hbm, g_ref, 4 * heads + 1)]
    load_q = by_head(q_hbm, q_ref, 2 * heads)
    load_do = by_head(do_hbm, do_ref, 3 * heads)
    for copy in load_k + load_v + load_small + load_q + load_do:
        copy.start()

    def signal(sem, at, core):
        pl.semaphore_signal(sem, inc=1, device_id=(at, core), device_id_type=MESH)

    def around(sem, radius):
        @pl.when(sp >= radius)
        def _():
            signal(sem, sp - radius, tp)

        @pl.when(sp < n_sp - radius)
        def _():
            signal(sem, sp + radius, tp)

    def count_around(radius):
        return jnp.where(sp >= radius, 1, 0) + jnp.where(sp < n_sp - radius, 1, 0)

    barrier = pltpu.get_barrier_semaphore()
    around(barrier, 1)
    for other in range(1, n_tp):
        signal(barrier, sp, lax.rem(tp + other, n_tp))
    pl.semaphore_wait(barrier, count_around(1) + n_tp - 1)

    rounds = []
    while 2 ** len(rounds) < n_sp:
        rounds.append(2 ** len(rounds))

    def say(step):
        around(hand_sem.at[step], rounds[step])

    def hear(step):
        pl.semaphore_wait(hand_sem.at[step], count_around(rounds[step]))

    def send(slot, src, dst, to):
        return pltpu.make_async_remote_copy(
            src_ref=src, dst_ref=dst, send_sem=send_sem.at[slot], recv_sem=recv_sem.at[slot],
            device_id=(to, tp), device_id_type=MESH,
        )

    k_next = [send(4 * h, k_ref.at[h], k_raw.at[h], nxt) for h in range(heads)]
    v_next = [send(4 * h + 1, v_ref.at[h], v_prev.at[h], nxt) for h in range(heads)]
    dv_back = [send(4 * h + 2, dv_out.at[h], dv_in.at[h], prv) for h in range(heads)]
    dk_back = [send(4 * h + 3, dk_out.at[h], dk_in.at[h], prv) for h in range(heads)]

    def start(gate, copies):
        @pl.when(gate)
        def _():
            for copy in copies:
                copy.start()

    for copy in load_k + load_v:
        copy.wait()
    yields = tp == n_tp - 1
    start(has_next, [k_next[0], v_next[0]])
    start(has_next & jnp.logical_not(yields), k_next[1:] + v_next[1:])
    say(0)
    for copy in load_small:
        copy.wait()

    @pl.when(jnp.logical_not(has_prev))
    def _():
        kn[:, 0:rows, :] = jnp.zeros((heads, rows, HEAD_DIM), BF16)
        v_prev[...] = jnp.zeros((heads, rows, HEAD_DIM), BF16)

    g0, g1 = g_ref[0:1, :], g_ref[1:2, :]
    low, high = slice(0, half), slice(half, rows)
    row = lax.broadcasted_iota(jnp.int32, (half, half), 0)
    col = lax.broadcasted_iota(jnp.int32, (half, half), 1)
    upper = col >= row
    absent = jnp.where(has_prev, 0.0, NEG)

    table = jnp.concatenate([t_ref[...], jnp.zeros((heads, 2 * half - entries), F32)], axis=1)
    table = pltpu.roll(table, 2 * half - lead, 1)
    for h in range(heads):
        def skew(line):
            return pltpu.roll(jnp.broadcast_to(line, (half, half)), 0, 1, stride=1, stride_axis=0)

        close = skew(table[h : h + 1, 0:half])
        ahead = skew(table[h : h + 1, half:])
        far = jnp.broadcast_to(table[h : h + 1, half : half + 1], (half, half))
        same = jnp.where(upper, close, ahead)
        same = jnp.where((row >= SEG) & (col < SEG), NEG, same)
        before = jnp.where(upper, far, close)
        distant = jnp.where((row < SEG) & (col >= SEG), NEG, far)
        top_own = jnp.max(same, axis=0, keepdims=True)
        top = jnp.maximum(top_own, jnp.max(before, axis=0, keepdims=True))
        first_top = jnp.where(has_prev, top, top_own)
        tiles[h, 0] = (same - first_top) * LOG2E
        tiles[h, 1] = (before - top) * LOG2E
        tiles[h, 2] = (same - top) * LOG2E
        tiles[h, 3] = (distant - top) * LOG2E + absent
        tiles[h, 4] = (before - top) * LOG2E + absent

    for h in range(heads):
        unit, rms = unit_of(k_ref[h])
        k_unit[h] = unit
        k_rms[h] = rms
        kn[h, rows:, :] = (unit * g1).astype(BF16)
    for copy in load_q + load_do:
        copy.wait()

    sums = []
    for h in range(heads):
        unit, rms = unit_of(q_ref[h])
        q_unit[h] = unit
        q_rms[h] = rms
        qn[h] = (unit * g0).astype(BF16)
        s0 = dot(kn[h, rows : rows + half, :], qn[h], (1, 1)) * scale
        s1 = dot(kn[h, rows + half :, :], qn[h, high, :], (1, 1)) * scale
        e0 = jnp.exp2(s0[:, low] + tiles[h, 0])
        e1 = jnp.exp2(s0[:, high] + tiles[h, 1])
        e2 = jnp.exp2(s1 + tiles[h, 2])
        e_own[h, 0], e_own[h, 1], e_own[h, 2] = e0, e1, e2
        p0 = dot(v_ref[h, low, :], do_ref[h], (1, 1))
        dp_own[h, 0], dp_own[h, 1] = p0[:, low], p0[:, high]
        dp_own[h, 2] = dot(v_ref[h, high, :], do_ref[h, high, :], (1, 1))
        sums.append((
            jnp.sum(e0, axis=0, keepdims=True),
            jnp.sum(e1, axis=0, keepdims=True) + jnp.sum(e2, axis=0, keepdims=True),
        ))
    step = 0

    def relay(step):
        if step < len(rounds):
            hear(step)
            if step + 1 < len(rounds):
                say(step + 1)
        return step + 1

    step = relay(step)
    step = relay(step)
    start(has_next & yields, k_next[1:] + v_next[1:])
    packed = []
    mass = jnp.zeros((1, HEAD_DIM), F32)
    for h in range(heads):
        @pl.when(has_prev)
        def _():
            k_next[h].wait_recv()
            kn[h, 0:rows, :] = (unit_of(k_raw[h])[0] * g1).astype(BF16)

        s0 = dot(kn[h, low, :], qn[h, low, :], (1, 1)) * scale
        s1 = dot(kn[h, high, :], qn[h], (1, 1)) * scale
        x0 = jnp.exp2(s0 + tiles[h, 3])
        x1 = jnp.exp2(s1[:, low] + tiles[h, 4])
        x2 = jnp.exp2(s1[:, high] + tiles[h, 3])
        r0 = 1.0 / (sums[h][0] + jnp.sum(x0 + x1, axis=0, keepdims=True))
        r1 = 1.0 / (sums[h][1] + jnp.sum(x2, axis=0, keepdims=True))
        x0, x1, x2 = x0 * r0, x1 * r0, x2 * r1
        e0, e1, e2 = e_own[h, 0] * r0, e_own[h, 1] * r1, e_own[h, 2] * r1
        d_o = do_ref[h]
        dv_out[h, low, :] = dot(x0.astype(BF16), d_o[low], (1, 0)).astype(BF16)
        dv_out[h, high, :] = dot(jnp.concatenate([x1, x2], axis=1).astype(BF16), d_o, (1, 0)).astype(BF16)
        dv_acc[h, low, :] = dot(jnp.concatenate([e0, e1], axis=1).astype(BF16), d_o, (1, 0))
        dv_acc[h, high, :] = dot(e2.astype(BF16), d_o[high], (1, 0))
        step = relay(step)
        own0 = jnp.sum(e0 * dp_own[h, 0], axis=0, keepdims=True)
        own1 = jnp.sum(e1 * dp_own[h, 1] + e2 * dp_own[h, 2], axis=0, keepdims=True)

        @pl.when(has_prev)
        def _():
            v_next[h].wait_recv()

        p0 = dot(v_prev[h, low, :], d_o[low], (1, 1))
        p1 = dot(v_prev[h, high, :], d_o, (1, 1))
        delta0 = own0 + jnp.sum(x0 * p0 + x1 * p1[:, low], axis=0, keepdims=True)
        delta1 = own1 + jnp.sum(x2 * p1[:, high], axis=0, keepdims=True)
        x0, x1, x2 = x0 * (p0 - delta0), x1 * (p1[:, low] - delta0), x2 * (p1[:, high] - delta1)
        e0, e1, e2 = e0 * (dp_own[h, 0] - delta0), e1 * (dp_own[h, 1] - delta1), e2 * (dp_own[h, 2] - delta1)
        blocks = [
            x0.astype(BF16),
            jnp.concatenate([x1, x2], axis=1).astype(BF16),
            jnp.concatenate([e0, e1], axis=1).astype(BF16),
            e2.astype(BF16),
        ]
        spans = [low, slice(0, rows), slice(0, rows), high]
        d_k = [dot(block, qn[h, span, :], (1, 0)) for block, span in zip(blocks, spans)]
        product = None
        for i, part in enumerate(d_k):
            term = part * kn[h, i * half : (i + 1) * half, :].astype(F32)
            product = term if product is None else product + term
        mass = mass + jnp.sum(product, axis=0, keepdims=True)
        same, before = e0 + e2, x1 + e1
        line_p = diagonals(jnp.where(upper, same, before), lead)
        line_n = diagonals(jnp.where(upper, 0.0, same), lead)
        lane = lax.broadcasted_iota(jnp.int32, line_p.shape, 1)
        rest = -(jnp.sum(line_p, axis=1, keepdims=True) + jnp.sum(line_n, axis=1, keepdims=True))
        packed.append(jnp.where(lane < lead, line_n, line_p))
        packed.append(jnp.where(lane < lead, line_p, jnp.where(lane == lead, rest, 0.0)))
        dk_out[h, low, :] = d_k[0].astype(BF16)
        dk_out[h, high, :] = d_k[1].astype(BF16)
        dk_acc[h, low, :] = d_k[2]
        dk_acc[h, high, :] = d_k[3]
        if h < heads - 1:
            start(has_prev, [dv_back[h], dk_back[h]])
        else:
            while step < len(rounds):
                step = relay(step)
            mass = mass * factor
            line_src[...] = mass
            one_src[...] = jnp.concatenate(
                packed + [mass, jnp.zeros((8 - 1 - len(packed), HEAD_DIM), F32)], axis=0
            )
            two[sp] = one_src[...]

            def spread(i):
                at = jnp.where(i >= sp, i + 1, i)
                pltpu.make_async_remote_copy(
                    src_ref=one_src, dst_ref=two.at[sp], send_sem=red_sem.at[0], recv_sem=red_sem.at[1],
                    device_id=(at, tp), device_id_type=MESH,
                ).start()

            def spread_line(at):
                for other in range(1, n_tp):
                    pltpu.make_async_remote_copy(
                        src_ref=line_src, dst_ref=lines.at[other - 1, sp], send_sem=red_sem.at[2],
                        recv_sem=red_sem.at[3], device_id=(at, lax.rem(tp + other, n_tp)), device_id_type=MESH,
                    ).start()

            if n_sp <= 32:
                for i in range(n_sp - 1):
                    spread(i)
                    spread_line(i)
                spread_line(n_sp - 1)
            else:
                @pl.loop(0, n_sp - 1)
                def _(i):
                    spread(i)

                @pl.loop(0, n_sp)
                def _(i):
                    spread_line(i)

            start(has_prev, [dv_back[h], dk_back[h]])
        for i, part in enumerate([
            dot(jnp.concatenate([blocks[0], blocks[1][:, low], blocks[2][:, low]], axis=0), kn[h, 0 : 3 * half, :], (0, 0)),
            dot(jnp.concatenate([blocks[1][:, high], blocks[2][:, high], blocks[3]], axis=0), kn[h, half:, :], (0, 0)),
        ]):
            span = slice(i * half, (i + 1) * half)
            grad = part * factor * g0
            unit = q_unit[h, span, :]
            out = q_rms[h, span, :] * (grad - unit * jnp.mean(grad * unit, axis=-1, keepdims=True))
            dq_ref[span, h * HEAD_DIM : (h + 1) * HEAD_DIM] = out.astype(BF16)

    for h in range(heads):
        across = slice(h * HEAD_DIM, (h + 1) * HEAD_DIM)

        @pl.when(has_next)
        def _():
            dv_back[h].wait_recv()
            dk_back[h].wait_recv()
            dv_acc[h] += dv_in[h].astype(F32)
            dk_acc[h] += dk_in[h].astype(F32)

        dv_ref[:, across] = dv_acc[h].astype(BF16)
        unit = k_unit[h]
        grad = dk_acc[h] * factor * g1
        out = k_rms[h] * (grad - unit * jnp.mean(grad * unit, axis=-1, keepdims=True))
        dk_ref[:, across] = out.astype(BF16)

    inverse = 1.0 / g_ref[...]
    peers = two.at[pl.ds(0, n_sp - 1)]
    pltpu.make_async_copy(peers, peers, red_sem.at[1]).wait()
    pltpu.make_async_copy(lines, lines, red_sem.at[3]).wait()
    whole = jnp.sum(two[...], axis=0)
    for h in range(heads):
        dt_ref[h : h + 1, 0:half] = whole[2 * h : 2 * h + 1]
        dt_ref[h : h + 1, half:] = whole[2 * h + 1 : 2 * h + 2, 0 : entries - half]
    mass = whole[2 * heads : 2 * heads + 1] + jnp.sum(lines[...], axis=(0, 1))
    dg_ref[...] = mass * inverse

    pltpu.make_async_copy(peers, peers, red_sem.at[0]).wait()
    pltpu.make_async_copy(lines, lines, red_sem.at[2]).wait()

    @pl.when(has_next)
    def _():
        for copy in k_next + v_next:
            copy.wait_send()

    @pl.when(has_prev)
    def _():
        for copy in dv_back + dk_back:
            copy.wait_send()


def emit(*refs):
    sem = refs[-1]
    count = len(refs) // 2
    copies = [pltpu.make_async_copy(refs[i], refs[count + i], sem.at[i]) for i in range(count)]
    for copy in copies:
        copy.start()
    for copy in copies:
        copy.wait()


def solution(mesh):
    n_sp, n_tp = mesh.shape["sp"], mesh.shape["tp"]

    def local(queries, keys, values, gains, bias_table, d_out):
        rows, width = queries.shape
        heads = width // HEAD_DIM
        half = rows // 2
        assert n_sp > 1 and rows == LEFT * SEG and half == MAX_REL == HEAD_DIM and 2 * heads + 1 <= 8
        act = jax.ShapeDtypeStruct((rows, width), BF16)
        vmem = pl.BlockSpec(memory_space=pltpu.VMEM)
        shapes = (
            act, act, act,
            jax.ShapeDtypeStruct(bias_table.shape[::-1], F32),
            jax.ShapeDtypeStruct(gains.shape, F32),
        )
        low = pltpu.VMEM((heads, rows, HEAD_DIM), BF16)
        wide = pltpu.VMEM((heads, rows, HEAD_DIM), F32)
        thin = pltpu.VMEM((heads, rows, 1), F32)
        parts = pl.pallas_call(
            functools.partial(kernel, n_sp, n_tp),
            out_shape=shapes,
            in_specs=[pl.BlockSpec(memory_space=pltpu.HBM)] * 6,
            out_specs=(vmem,) * 5,
            scratch_shapes=[
                low, low, low, low,
                pltpu.VMEM(gains.shape, F32),
                pltpu.VMEM(bias_table.shape[::-1], F32),
                low, low,
                pltpu.VMEM((heads, 2 * rows, HEAD_DIM), BF16),
                low,
                wide, thin, wide, thin,
                pltpu.VMEM((heads, 5, half, half), F32),
                pltpu.VMEM((heads, 3, half, half), F32),
                pltpu.VMEM((heads, 3, half, half), F32),
                wide, wide,
                low, low, low, low,
                pltpu.VMEM((8, HEAD_DIM), F32),
                pltpu.VMEM((n_sp, 8, HEAD_DIM), F32),
                pltpu.VMEM((1, HEAD_DIM), F32),
                pltpu.VMEM((n_tp - 1, n_sp, 1, HEAD_DIM), F32),
                pltpu.SemaphoreType.DMA((4 * heads + 2,)),
                pltpu.SemaphoreType.DMA((4 * heads,)),
                pltpu.SemaphoreType.DMA((4 * heads,)),
                pltpu.SemaphoreType.DMA((4,)),
                pltpu.SemaphoreType.REGULAR((max(1, (n_sp - 1).bit_length()),)),
            ],
            compiler_params=pltpu.CompilerParams(
                collective_id=0, has_side_effects=True, vmem_limit_bytes=24 * 1024 * 1024
            ),
        )(*(
            pltpu.with_memory_space_constraint(x, pltpu.HBM)
            for x in (queries, keys, values, d_out, gains, bias_table.T)
        ))
        d_q, d_k, d_v, d_table, d_gains = pl.pallas_call(
            emit,
            out_shape=shapes,
            in_specs=[vmem] * 5,
            out_specs=(pl.BlockSpec(memory_space=pltpu.HBM),) * 5,
            scratch_shapes=[pltpu.SemaphoreType.DMA((5,))],
            compiler_params=pltpu.CompilerParams(vmem_limit_bytes=8 * 1024 * 1024),
        )(*parts)
        return d_q, d_k, d_v, d_table.T, d_gains

    in_specs = (P("sp", "tp"), P("sp", "tp"), P("sp", "tp"), P(), P(None, "tp"), P("sp", "tp"))
    out_specs = (P("sp", "tp"), P("sp", "tp"), P("sp", "tp"), P(None, "tp"), P())
    return jax.shard_map(local, mesh=mesh, in_specs=in_specs, out_specs=out_specs, check_vma=False)
```

```python
import functools

import jax
import jax.numpy as jnp
from jax import lax
from jax.experimental import pallas as pl
from jax.experimental.pallas import tpu as pltpu
from jax.sharding import PartitionSpec as P

HEAD_DIM = 128
SEG = 64
LEFT = 4
MAX_REL = 128
EPSILON = 1e-06
NEG = -1e30
LOG2E = 1.4426950408889634
MESH = pl.DeviceIdType.MESH
F32 = jnp.float32
BF16 = jnp.bfloat16


def dot(a, b, contract):
    return lax.dot_general(a, b, ((contract[:1], contract[1:]), ((), ())), preferred_element_type=F32)


def unit_of(block):
    wide = block.astype(F32)
    rms = lax.rsqrt(jnp.mean(wide * wide, axis=-1, keepdims=True) + EPSILON)
    return wide * rms, rms


def diagonals(tile, lead):
    rows, lanes = tile.shape
    total = None
    for start in range(0, rows, 8):
        turned = pltpu.roll(tile[start : start + 8], (lead - start) % lanes, 1)
        total = turned if total is None else total + turned
    sublane = lax.broadcasted_iota(jnp.int32, total.shape, 0)
    line = jnp.where(sublane == 0, total, 0.0)
    for i in range(1, 8):
        line = line + jnp.where(sublane == i, pltpu.roll(total, lanes - i, 1), 0.0)
    return jnp.sum(line, axis=0, keepdims=True)


def kernel(
    n_sp, n_tp,
    q_hbm, k_hbm, v_hbm, do_hbm, g_hbm, t_hbm,
    dq_ref, dk_ref, dv_ref, dt_ref, dg_ref,
    q_ref, k_ref, v_ref, do_ref, g_ref, t_ref, k_raw, v_prev, kn, qn, q_unit, q_rms, k_unit, k_rms,
    tiles, e_own, dp_own, dk_acc, dv_acc, dk_out, dv_out, dk_in, dv_in, one_src, two, line_src, lines,
    load_sem, send_sem, recv_sem, red_sem, hand_sem,
):
    heads, rows, _ = q_ref.shape
    half = rows // 2
    entries = t_ref.shape[1]
    lead = SEG - 1
    factor = HEAD_DIM ** (-0.5)
    scale = factor * LOG2E
    sp, tp = lax.axis_index("sp"), lax.axis_index("tp")
    has_prev, has_next = sp > 0, sp < n_sp - 1
    nxt, prv = sp + 1, sp - 1

    def load(src, dst, slot):
        return pltpu.make_async_copy(src, dst, load_sem.at[slot])

    def by_head(src, dst, slot):
        return [load(src.at[:, pl.ds(h * HEAD_DIM, HEAD_DIM)], dst.at[h], slot + h) for h in range(heads)]

    load_k = by_head(k_hbm, k_ref, 0)
    load_v = by_head(v_hbm, v_ref, heads)
    load_small = [load(t_hbm, t_ref, 4 * heads), load(g_hbm, g_ref, 4 * heads + 1)]
    load_q = by_head(q_hbm, q_ref, 2 * heads)
    load_do = by_head(do_hbm, do_ref, 3 * heads)
    for copy in load_k + load_v + load_small + load_q + load_do:
        copy.start()

    def signal(sem, at, core):
        pl.semaphore_signal(sem, inc=1, device_id=(at, core), device_id_type=MESH)

    def around(sem, radius):
        @pl.when(sp >= radius)
        def _():
            signal(sem, sp - radius, tp)

        @pl.when(sp < n_sp - radius)
        def _():
            signal(sem, sp + radius, tp)

    def count_around(radius):
        return jnp.where(sp >= radius, 1, 0) + jnp.where(sp < n_sp - radius, 1, 0)

    barrier = pltpu.get_barrier_semaphore()
    around(barrier, 1)
    for other in range(1, n_tp):
        signal(barrier, sp, lax.rem(tp + other, n_tp))
    pl.semaphore_wait(barrier, count_around(1) + n_tp - 1)

    rounds = []
    while 2 ** len(rounds) < n_sp:
        rounds.append(2 ** len(rounds))

    def say(step):
        around(hand_sem.at[step], rounds[step])

    def hear(step):
        pl.semaphore_wait(hand_sem.at[step], count_around(rounds[step]))

    def send(slot, src, dst, to):
        return pltpu.make_async_remote_copy(
            src_ref=src, dst_ref=dst, send_sem=send_sem.at[slot], recv_sem=recv_sem.at[slot],
            device_id=(to, tp), device_id_type=MESH,
        )

    k_next = [send(4 * h, k_ref.at[h], k_raw.at[h], nxt) for h in range(heads)]
    v_next = [send(4 * h + 1, v_ref.at[h], v_prev.at[h], nxt) for h in range(heads)]
    dv_back = [send(4 * h + 2, dv_out.at[h], dv_in.at[h], prv) for h in range(heads)]
    dk_back = [send(4 * h + 3, dk_out.at[h], dk_in.at[h], prv) for h in range(heads)]

    def start(gate, copies):
        @pl.when(gate)
        def _():
            for copy in copies:
                copy.start()

    for copy in load_k + load_v:
        copy.wait()
    yields = tp == n_tp - 1
    eager = sp < n_sp // 4
    start(has_next, [k_next[0], v_next[0]])
    start(has_next & jnp.logical_not(yields), k_next[1:] + v_next[1:])
    say(0)
    for copy in load_small:
        copy.wait()

    @pl.when(jnp.logical_not(has_prev))
    def _():
        kn[:, 0:rows, :] = jnp.zeros((heads, rows, HEAD_DIM), BF16)
        v_prev[...] = jnp.zeros((heads, rows, HEAD_DIM), BF16)

    g0, g1 = g_ref[0:1, :], g_ref[1:2, :]
    low, high = slice(0, half), slice(half, rows)
    row = lax.broadcasted_iota(jnp.int32, (half, half), 0)
    col = lax.broadcasted_iota(jnp.int32, (half, half), 1)
    upper = col >= row
    absent = jnp.where(has_prev, 0.0, NEG)

    table = jnp.concatenate([t_ref[...], jnp.zeros((heads, 2 * half - entries), F32)], axis=1)
    table = pltpu.roll(table, 2 * half - lead, 1)
    for h in range(heads):
        def skew(line):
            return pltpu.roll(jnp.broadcast_to(line, (half, half)), 0, 1, stride=1, stride_axis=0)

        close = skew(table[h : h + 1, 0:half])
        ahead = skew(table[h : h + 1, half:])
        far = jnp.broadcast_to(table[h : h + 1, half : half + 1], (half, half))
        same = jnp.where(upper, close, ahead)
        same = jnp.where((row >= SEG) & (col < SEG), NEG, same)
        before = jnp.where(upper, far, close)
        distant = jnp.where((row < SEG) & (col >= SEG), NEG, far)
        top_own = jnp.max(same, axis=0, keepdims=True)
        top = jnp.maximum(top_own, jnp.max(before, axis=0, keepdims=True))
        first_top = jnp.where(has_prev, top, top_own)
        tiles[h, 0] = (same - first_top) * LOG2E
        tiles[h, 1] = (before - top) * LOG2E
        tiles[h, 2] = (same - top) * LOG2E
        tiles[h, 3] = (distant - top) * LOG2E + absent
        tiles[h, 4] = (before - top) * LOG2E + absent

    for h in range(heads):
        unit, rms = unit_of(k_ref[h])
        k_unit[h] = unit
        k_rms[h] = rms
        kn[h, rows:, :] = (unit * g1).astype(BF16)
    for copy in load_q + load_do:
        copy.wait()

    sums = []
    for h in range(heads):
        unit, rms = unit_of(q_ref[h])
        q_unit[h] = unit
        q_rms[h] = rms
        qn[h] = (unit * g0).astype(BF16)
        s0 = dot(kn[h, rows : rows + half, :], qn[h], (1, 1)) * scale
        s1 = dot(kn[h, rows + half :, :], qn[h, high, :], (1, 1)) * scale
        e0 = jnp.exp2(s0[:, low] + tiles[h, 0])
        e1 = jnp.exp2(s0[:, high] + tiles[h, 1])
        e2 = jnp.exp2(s1 + tiles[h, 2])
        e_own[h, 0], e_own[h, 1], e_own[h, 2] = e0, e1, e2
        p0 = dot(v_ref[h, low, :], do_ref[h], (1, 1))
        dp_own[h, 0], dp_own[h, 1] = p0[:, low], p0[:, high]
        dp_own[h, 2] = dot(v_ref[h, high, :], do_ref[h, high, :], (1, 1))
        sums.append((
            jnp.sum(e0, axis=0, keepdims=True),
            jnp.sum(e1, axis=0, keepdims=True) + jnp.sum(e2, axis=0, keepdims=True),
        ))
    step = 0

    def relay(step):
        if step < len(rounds):
            hear(step)
            if step + 1 < len(rounds):
                say(step + 1)
        return step + 1

    step = relay(step)
    step = relay(step)
    packed = []
    mass = jnp.zeros((1, HEAD_DIM), F32)
    for h in range(heads):
        @pl.when(has_prev)
        def _():
            k_next[h].wait_recv()
            kn[h, 0:rows, :] = (unit_of(k_raw[h])[0] * g1).astype(BF16)

        s0 = dot(kn[h, low, :], qn[h, low, :], (1, 1)) * scale
        s1 = dot(kn[h, high, :], qn[h], (1, 1)) * scale
        x0 = jnp.exp2(s0 + tiles[h, 3])
        x1 = jnp.exp2(s1[:, low] + tiles[h, 4])
        x2 = jnp.exp2(s1[:, high] + tiles[h, 3])
        r0 = 1.0 / (sums[h][0] + jnp.sum(x0 + x1, axis=0, keepdims=True))
        r1 = 1.0 / (sums[h][1] + jnp.sum(x2, axis=0, keepdims=True))
        x0, x1, x2 = x0 * r0, x1 * r0, x2 * r1
        e0, e1, e2 = e_own[h, 0] * r0, e_own[h, 1] * r1, e_own[h, 2] * r1
        d_o = do_ref[h]
        dv_out[h, low, :] = dot(x0.astype(BF16), d_o[low], (1, 0)).astype(BF16)
        dv_out[h, high, :] = dot(jnp.concatenate([x1, x2], axis=1).astype(BF16), d_o, (1, 0)).astype(BF16)
        dv_acc[h, low, :] = dot(jnp.concatenate([e0, e1], axis=1).astype(BF16), d_o, (1, 0))
        dv_acc[h, high, :] = dot(e2.astype(BF16), d_o[high], (1, 0))
        if h == 0:
            start(has_next & yields, k_next[1:])
        if step < len(rounds) - 1:
            step = relay(step)
        if h == 0:
            start(has_next & yields, v_next[1:])
        own0 = jnp.sum(e0 * dp_own[h, 0], axis=0, keepdims=True)
        own1 = jnp.sum(e1 * dp_own[h, 1] + e2 * dp_own[h, 2], axis=0, keepdims=True)

        @pl.when(has_prev)
        def _():
            v_next[h].wait_recv()

        p0 = dot(v_prev[h, low, :], d_o[low], (1, 1))
        p1 = dot(v_prev[h, high, :], d_o, (1, 1))
        delta0 = own0 + jnp.sum(x0 * p0 + x1 * p1[:, low], axis=0, keepdims=True)
        delta1 = own1 + jnp.sum(x2 * p1[:, high], axis=0, keepdims=True)
        x0, x1, x2 = x0 * (p0 - delta0), x1 * (p1[:, low] - delta0), x2 * (p1[:, high] - delta1)
        e0, e1, e2 = e0 * (dp_own[h, 0] - delta0), e1 * (dp_own[h, 1] - delta1), e2 * (dp_own[h, 2] - delta1)
        blocks = [
            x0.astype(BF16),
            jnp.concatenate([x1, x2], axis=1).astype(BF16),
            jnp.concatenate([e0, e1], axis=1).astype(BF16),
            e2.astype(BF16),
        ]
        spans = [low, slice(0, rows), slice(0, rows), high]
        d_k = [dot(block, qn[h, span, :], (1, 0)) for block, span in zip(blocks, spans)]
        product = None
        for i, part in enumerate(d_k):
            term = part * kn[h, i * half : (i + 1) * half, :].astype(F32)
            product = term if product is None else product + term
        mass = mass + jnp.sum(product, axis=0, keepdims=True)
        same, before = e0 + e2, x1 + e1
        line_p = diagonals(jnp.where(upper, same, before), lead)
        line_n = diagonals(jnp.where(upper, 0.0, same), lead)
        lane = lax.broadcasted_iota(jnp.int32, line_p.shape, 1)
        rest = -(jnp.sum(line_p, axis=1, keepdims=True) + jnp.sum(line_n, axis=1, keepdims=True))
        packed.append(jnp.where(lane < lead, line_n, line_p))
        packed.append(jnp.where(lane < lead, line_p, jnp.where(lane == lead, rest, 0.0)))
        dk_out[h, low, :] = d_k[0].astype(BF16)
        dk_out[h, high, :] = d_k[1].astype(BF16)
        dk_acc[h, low, :] = d_k[2]
        dk_acc[h, high, :] = d_k[3]
        if h < heads - 1:
            start(has_prev, [dv_back[h], dk_back[h]])
        else:
            mass = mass * factor
            line_src[...] = mass
            one_src[...] = jnp.concatenate(
                packed + [mass, jnp.zeros((8 - 1 - len(packed), HEAD_DIM), F32)], axis=0
            )
            two[sp] = one_src[...]

            def spread(i):
                at = jnp.where(i >= sp, i + 1, i)
                pltpu.make_async_remote_copy(
                    src_ref=one_src, dst_ref=two.at[sp], send_sem=red_sem.at[0], recv_sem=red_sem.at[1],
                    device_id=(at, tp), device_id_type=MESH,
                ).start()

            def spread_line(at):
                for other in range(1, n_tp):
                    pltpu.make_async_remote_copy(
                        src_ref=line_src, dst_ref=lines.at[other - 1, sp], send_sem=red_sem.at[2],
                        recv_sem=red_sem.at[3], device_id=(at, lax.rem(tp + other, n_tp)), device_id_type=MESH,
                    ).start()

            def publish():
                for late in range(step, len(rounds)):
                    relay(late)
                if n_sp <= 32:
                    for i in range(n_sp - 1):
                        spread(i)
                        spread_line(i)
                    spread_line(n_sp - 1)
                else:
                    @pl.loop(0, n_sp - 1)
                    def _(i):
                        spread(i)

                    @pl.loop(0, n_sp)
                    def _(i):
                        spread_line(i)

            @pl.when(jnp.logical_not(eager))
            def _():
                publish()

            start(has_prev & jnp.logical_not(yields), [dk_back[h], dv_back[h]])
        for i, part in enumerate([
            dot(jnp.concatenate([blocks[0], blocks[1][:, low], blocks[2][:, low]], axis=0), kn[h, 0 : 3 * half, :], (0, 0)),
            dot(jnp.concatenate([blocks[1][:, high], blocks[2][:, high], blocks[3]], axis=0), kn[h, half:, :], (0, 0)),
        ]):
            span = slice(i * half, (i + 1) * half)
            grad = part * factor * g0
            unit = q_unit[h, span, :]
            out = q_rms[h, span, :] * (grad - unit * jnp.mean(grad * unit, axis=-1, keepdims=True))
            dq_ref[span, h * HEAD_DIM : (h + 1) * HEAD_DIM] = out.astype(BF16)

    @pl.when(eager)
    def _():
        publish()

    def add_dv(h):
        @pl.when(has_next)
        def _():
            dv_acc[h] += dv_in[h].astype(F32)

        dv_ref[:, h * HEAD_DIM : (h + 1) * HEAD_DIM] = dv_acc[h].astype(BF16)

    for h in range(heads):
        across = slice(h * HEAD_DIM, (h + 1) * HEAD_DIM)

        @pl.when(has_next)
        def _():
            (dv_back if h < heads - 1 else dk_back)[h].wait_recv()

        if h == 0:
            start(has_prev & yields, [dk_back[heads - 1], dv_back[heads - 1]])
        if h < heads - 1:
            add_dv(h)

            @pl.when(has_next)
            def _():
                dk_back[h].wait_recv()

        @pl.when(has_next)
        def _():
            dk_acc[h] += dk_in[h].astype(F32)

        unit = k_unit[h]
        grad = dk_acc[h] * factor * g1
        out = k_rms[h] * (grad - unit * jnp.mean(grad * unit, axis=-1, keepdims=True))
        dk_ref[:, across] = out.astype(BF16)
        if h == heads - 1:
            @pl.when(has_next)
            def _():
                dv_back[h].wait_recv()

            add_dv(h)

    inverse = 1.0 / g_ref[...]
    peers = two.at[pl.ds(0, n_sp - 1)]
    pltpu.make_async_copy(peers, peers, red_sem.at[1]).wait()
    pltpu.make_async_copy(lines, lines, red_sem.at[3]).wait()
    whole = jnp.sum(two[...], axis=0)
    for h in range(heads):
        dt_ref[h : h + 1, 0:half] = whole[2 * h : 2 * h + 1]
        dt_ref[h : h + 1, half:] = whole[2 * h + 1 : 2 * h + 2, 0 : entries - half]
    mass = whole[2 * heads : 2 * heads + 1] + jnp.sum(lines[...], axis=(0, 1))
    dg_ref[...] = mass * inverse

    pltpu.make_async_copy(peers, peers, red_sem.at[0]).wait()
    pltpu.make_async_copy(lines, lines, red_sem.at[2]).wait()

    @pl.when(has_next)
    def _():
        for copy in k_next + v_next:
            copy.wait_send()

    @pl.when(has_prev)
    def _():
        for copy in dv_back + dk_back:
            copy.wait_send()


def emit(*refs):
    sem = refs[-1]
    count = len(refs) // 2
    copies = [pltpu.make_async_copy(refs[i], refs[count + i], sem.at[i]) for i in range(count)]
    for copy in copies:
        copy.start()
    for copy in copies:
        copy.wait()


def solution(mesh):
    n_sp, n_tp = mesh.shape["sp"], mesh.shape["tp"]

    def local(queries, keys, values, gains, bias_table, d_out):
        rows, width = queries.shape
        heads = width // HEAD_DIM
        half = rows // 2
        assert n_sp > 1 and rows == LEFT * SEG and half == MAX_REL == HEAD_DIM and 2 * heads + 1 <= 8
        act = jax.ShapeDtypeStruct((rows, width), BF16)
        vmem = pl.BlockSpec(memory_space=pltpu.VMEM)
        shapes = (
            act, act, act,
            jax.ShapeDtypeStruct(bias_table.shape[::-1], F32),
            jax.ShapeDtypeStruct(gains.shape, F32),
        )
        low = pltpu.VMEM((heads, rows, HEAD_DIM), BF16)
        wide = pltpu.VMEM((heads, rows, HEAD_DIM), F32)
        thin = pltpu.VMEM((heads, rows, 1), F32)
        parts = pl.pallas_call(
            functools.partial(kernel, n_sp, n_tp),
            out_shape=shapes,
            in_specs=[pl.BlockSpec(memory_space=pltpu.HBM)] * 6,
            out_specs=(vmem,) * 5,
            scratch_shapes=[
                low, low, low, low,
                pltpu.VMEM(gains.shape, F32),
                pltpu.VMEM(bias_table.shape[::-1], F32),
                low, low,
                pltpu.VMEM((heads, 2 * rows, HEAD_DIM), BF16),
                low,
                wide, thin, wide, thin,
                pltpu.VMEM((heads, 5, half, half), F32),
                pltpu.VMEM((heads, 3, half, half), F32),
                pltpu.VMEM((heads, 3, half, half), F32),
                wide, wide,
                low, low, low, low,
                pltpu.VMEM((8, HEAD_DIM), F32),
                pltpu.VMEM((n_sp, 8, HEAD_DIM), F32),
                pltpu.VMEM((1, HEAD_DIM), F32),
                pltpu.VMEM((n_tp - 1, n_sp, 1, HEAD_DIM), F32),
                pltpu.SemaphoreType.DMA((4 * heads + 2,)),
                pltpu.SemaphoreType.DMA((4 * heads,)),
                pltpu.SemaphoreType.DMA((4 * heads,)),
                pltpu.SemaphoreType.DMA((4,)),
                pltpu.SemaphoreType.REGULAR((max(1, (n_sp - 1).bit_length()),)),
            ],
            compiler_params=pltpu.CompilerParams(
                collective_id=0, has_side_effects=True, vmem_limit_bytes=24 * 1024 * 1024
            ),
        )(*(
            pltpu.with_memory_space_constraint(x, pltpu.HBM)
            for x in (queries, keys, values, d_out, gains, bias_table.T)
        ))
        d_q, d_k, d_v, d_table, d_gains = pl.pallas_call(
            emit,
            out_shape=shapes,
            in_specs=[vmem] * 5,
            out_specs=(pl.BlockSpec(memory_space=pltpu.HBM),) * 5,
            scratch_shapes=[pltpu.SemaphoreType.DMA((5,))],
            compiler_params=pltpu.CompilerParams(vmem_limit_bytes=8 * 1024 * 1024),
        )(*parts)
        return d_q, d_k, d_v, d_table.T, d_gains

    in_specs = (P("sp", "tp"), P("sp", "tp"), P("sp", "tp"), P(), P(None, "tp"), P("sp", "tp"))
    out_specs = (P("sp", "tp"), P("sp", "tp"), P("sp", "tp"), P(None, "tp"), P())
    return jax.shard_map(local, mesh=mesh, in_specs=in_specs, out_specs=out_specs, check_vma=False)
```

```python
import functools

import jax
import jax.numpy as jnp
from jax import lax
from jax.experimental import pallas as pl
from jax.experimental.pallas import tpu as pltpu
from jax.sharding import PartitionSpec as P

HEAD_DIM = 128
SEG = 64
LEFT = 4
MAX_REL = 128
EPSILON = 1e-06
NEG = -1e30
LOG2E = 1.4426950408889634
MESH = pl.DeviceIdType.MESH
F32 = jnp.float32
BF16 = jnp.bfloat16


def dot(a, b, contract):
    return lax.dot_general(a, b, ((contract[:1], contract[1:]), ((), ())), preferred_element_type=F32)


def unit_of(block):
    wide = block.astype(F32)
    rms = lax.rsqrt(jnp.mean(wide * wide, axis=-1, keepdims=True) + EPSILON)
    return wide * rms, rms


def fold(tile, lead):
    total = None
    for start in range(0, tile.shape[0], 8):
        turned = pltpu.roll(tile[start : start + 8], (lead - start) % tile.shape[1], 1)
        total = turned if total is None else total + turned
    return total


def align(total):
    lanes = total.shape[1]
    sublane = lax.broadcasted_iota(jnp.int32, total.shape, 0)
    line = jnp.where(sublane == 0, total, 0.0)
    for i in range(1, 8):
        line = line + jnp.where(sublane == i, pltpu.roll(total, lanes - i, 1), 0.0)
    return jnp.sum(line, axis=0, keepdims=True)


def kernel(
    n_sp, n_tp,
    q_hbm, k_hbm, v_hbm, do_hbm, g_hbm, t_hbm,
    dq_ref, dk_ref, dv_ref, dt_ref, dg_ref,
    kv_ref, qd_ref, g_ref, t_ref, k_raw, v_prev, kn, qn, q_unit, q_rms, k_unit, k_rms,
    tiles, e_own, dp_own, dk_acc, dv_acc, out_ref, dk_in, dv_in, one_src, two, line_src, lines,
    load_sem, send_sem, recv_sem, red_sem, hand_sem,
):
    heads, rows, _ = k_raw.shape
    k_ref, v_ref = kv_ref.at[pl.ds(0, heads)], kv_ref.at[pl.ds(heads, heads)]
    q_ref, do_ref = qd_ref.at[pl.ds(0, heads)], qd_ref.at[pl.ds(heads, heads)]
    dk_out, dv_out = out_ref.at[pl.ds(0, heads)], out_ref.at[pl.ds(heads, heads)]
    half = rows // 2
    entries = t_ref.shape[1]
    lead = SEG - 1
    factor = HEAD_DIM ** (-0.5)
    scale = factor * LOG2E
    sp, tp = lax.axis_index("sp"), lax.axis_index("tp")
    has_prev, has_next = sp > 0, sp < n_sp - 1
    nxt, prv = sp + 1, sp - 1

    def load(src, dst, slot):
        return pltpu.make_async_copy(src, dst, load_sem.at[slot])

    def by_head(src, dst, slot):
        return [load(src.at[:, pl.ds(h * HEAD_DIM, HEAD_DIM)], dst.at[h], slot) for h in range(heads)]

    def drain(ref, sem):
        pltpu.make_async_copy(ref, ref, sem).wait()

    load_small = [load(t_hbm, t_ref, 2), load(g_hbm, g_ref, 3)]
    for copy in (
        by_head(k_hbm, k_ref, 0) + by_head(v_hbm, v_ref, 0) + load_small
        + by_head(q_hbm, q_ref, 1) + by_head(do_hbm, do_ref, 1)
    ):
        copy.start()

    def signal(sem, at, core):
        pl.semaphore_signal(sem, inc=1, device_id=(at, core), device_id_type=MESH)

    def around(sem, radius):
        @pl.when(sp >= radius)
        def _():
            signal(sem, sp - radius, tp)

        @pl.when(sp < n_sp - radius)
        def _():
            signal(sem, sp + radius, tp)

    def count_around(radius):
        return jnp.where(sp >= radius, 1, 0) + jnp.where(sp < n_sp - radius, 1, 0)

    barrier = pltpu.get_barrier_semaphore()
    around(barrier, 1)
    for other in range(1, n_tp):
        signal(barrier, sp, lax.rem(tp + other, n_tp))
    pl.semaphore_wait(barrier, count_around(1) + n_tp - 1)

    rounds = []
    while 2 ** len(rounds) < n_sp:
        rounds.append(2 ** len(rounds))

    def say(step):
        around(hand_sem.at[step], rounds[step])

    def hear(step):
        pl.semaphore_wait(hand_sem.at[step], count_around(rounds[step]))

    def send(slot, src, dst, to):
        return pltpu.make_async_remote_copy(
            src_ref=src, dst_ref=dst, send_sem=send_sem.at[slot % 4 // 2], recv_sem=recv_sem.at[slot],
            device_id=(to, tp), device_id_type=MESH,
        )

    k_next = [send(4 * h, k_ref.at[h], k_raw.at[h], nxt) for h in range(heads)]
    v_next = [send(4 * h + 1, v_ref.at[h], v_prev.at[h], nxt) for h in range(heads)]
    dv_back = [send(4 * h + 2, dv_out.at[h], dv_in.at[h], prv) for h in range(heads)]
    dk_back = [send(4 * h + 3, dk_out.at[h], dk_in.at[h], prv) for h in range(heads)]

    def start(gate, copies):
        @pl.when(gate)
        def _():
            for copy in copies:
                copy.start()

    drain(kv_ref, load_sem.at[0])
    yields = tp == n_tp - 1
    eager = sp < n_sp // 4
    start(has_next, [k_next[0], v_next[0]])
    start(has_next & jnp.logical_not(yields), k_next[1:] + v_next[1:])
    say(0)
    for copy in load_small:
        copy.wait()

    @pl.when(jnp.logical_not(has_prev))
    def _():
        kn[:, 0:rows, :] = jnp.zeros((heads, rows, HEAD_DIM), BF16)
        v_prev[...] = jnp.zeros((heads, rows, HEAD_DIM), BF16)

    g0, g1 = g_ref[0:1, :], g_ref[1:2, :]
    low, high = slice(0, half), slice(half, rows)
    row = lax.broadcasted_iota(jnp.int32, (half, half), 0)
    col = lax.broadcasted_iota(jnp.int32, (half, half), 1)
    upper = col >= row
    absent = jnp.where(has_prev, 0.0, NEG)

    table = jnp.concatenate([t_ref[...], jnp.zeros((heads, 2 * half - entries), F32)], axis=1)
    table = pltpu.roll(table, 2 * half - lead, 1)
    for h in range(heads):
        def skew(line):
            return pltpu.roll(jnp.broadcast_to(line, (half, half)), 0, 1, stride=1, stride_axis=0)

        close = skew(table[h : h + 1, 0:half])
        ahead = skew(table[h : h + 1, half:])
        far = jnp.broadcast_to(table[h : h + 1, half : half + 1], (half, half))
        same = jnp.where(upper, close, ahead)
        same = jnp.where((row >= SEG) & (col < SEG), NEG, same)
        before = jnp.where(upper, far, close)
        distant = jnp.where((row < SEG) & (col >= SEG), NEG, far)
        top_own = jnp.max(same, axis=0, keepdims=True)
        top = jnp.maximum(top_own, jnp.max(before, axis=0, keepdims=True))
        first_top = jnp.where(has_prev, top, top_own)
        tiles[h, 0] = (same - first_top) * LOG2E
        tiles[h, 1] = (before - top) * LOG2E
        tiles[h, 2] = (same - top) * LOG2E
        tiles[h, 3] = (distant - top) * LOG2E + absent
        tiles[h, 4] = (before - top) * LOG2E + absent

    inverse = 1.0 / g_ref[...]
    for h in range(heads):
        unit, rms = unit_of(k_ref[h])
        k_unit[h] = unit
        k_rms[h] = rms
        kn[h, rows:, :] = (unit * g1).astype(BF16)
    drain(qd_ref, load_sem.at[1])

    sums = []
    for h in range(heads):
        unit, rms = unit_of(q_ref[h])
        q_unit[h] = unit
        q_rms[h] = rms
        qn[h] = (unit * g0).astype(BF16)
        s0 = dot(kn[h, rows : rows + half, :], qn[h], (1, 1)) * scale
        s1 = dot(kn[h, rows + half :, :], qn[h, high, :], (1, 1)) * scale
        e0 = jnp.exp2(s0[:, low] + tiles[h, 0])
        e1 = jnp.exp2(s0[:, high] + tiles[h, 1])
        e2 = jnp.exp2(s1 + tiles[h, 2])
        e_own[h, 0], e_own[h, 1], e_own[h, 2] = e0, e1, e2
        p0 = dot(v_ref[h, low, :], do_ref[h], (1, 1))
        dp_own[h, 0], dp_own[h, 1] = p0[:, low], p0[:, high]
        dp_own[h, 2] = dot(v_ref[h, high, :], do_ref[h, high, :], (1, 1))
        sums.append((
            jnp.sum(e0, axis=0, keepdims=True),
            jnp.sum(e1, axis=0, keepdims=True) + jnp.sum(e2, axis=0, keepdims=True),
        ))
    step = 0

    def relay(step):
        if step < len(rounds):
            hear(step)
            if step + 1 < len(rounds):
                say(step + 1)
        return step + 1

    step = relay(step)
    step = relay(step)
    packed = []
    mass = jnp.zeros((1, HEAD_DIM), F32)
    for h in range(heads):
        @pl.when(has_prev)
        def _():
            k_next[h].wait_recv()
            kn[h, 0:rows, :] = (unit_of(k_raw[h])[0] * g1).astype(BF16)

        s0 = dot(kn[h, low, :], qn[h, low, :], (1, 1)) * scale
        s1 = dot(kn[h, high, :], qn[h], (1, 1)) * scale
        x0 = jnp.exp2(s0 + tiles[h, 3])
        x1 = jnp.exp2(s1[:, low] + tiles[h, 4])
        x2 = jnp.exp2(s1[:, high] + tiles[h, 3])
        r0 = 1.0 / (sums[h][0] + jnp.sum(x0 + x1, axis=0, keepdims=True))
        r1 = 1.0 / (sums[h][1] + jnp.sum(x2, axis=0, keepdims=True))
        x0, x1, x2 = x0 * r0, x1 * r0, x2 * r1
        e0, e1, e2 = e_own[h, 0] * r0, e_own[h, 1] * r1, e_own[h, 2] * r1
        d_o = do_ref[h]
        dv_out[h, low, :] = dot(x0.astype(BF16), d_o[low], (1, 0)).astype(BF16)
        dv_out[h, high, :] = dot(jnp.concatenate([x1, x2], axis=1).astype(BF16), d_o, (1, 0)).astype(BF16)
        dv_acc[h, low, :] = dot(jnp.concatenate([e0, e1], axis=1).astype(BF16), d_o, (1, 0))
        dv_acc[h, high, :] = dot(e2.astype(BF16), d_o[high], (1, 0))
        if h == 0:
            start(has_next & yields, k_next[1:])
        if h == heads - 1:
            start(has_prev & jnp.logical_not(yields), [dv_back[h]])
        if step < len(rounds) - 1:
            step = relay(step)
        if h == 0:
            start(has_next & yields, v_next[1:])
        own0 = jnp.sum(e0 * dp_own[h, 0], axis=0, keepdims=True)
        own1 = jnp.sum(e1 * dp_own[h, 1] + e2 * dp_own[h, 2], axis=0, keepdims=True)

        @pl.when(has_prev)
        def _():
            v_next[h].wait_recv()

        p0 = dot(v_prev[h, low, :], d_o[low], (1, 1))
        p1 = dot(v_prev[h, high, :], d_o, (1, 1))
        delta0 = own0 + jnp.sum(x0 * p0 + x1 * p1[:, low], axis=0, keepdims=True)
        delta1 = own1 + jnp.sum(x2 * p1[:, high], axis=0, keepdims=True)
        x0, x1, x2 = x0 * (p0 - delta0), x1 * (p1[:, low] - delta0), x2 * (p1[:, high] - delta1)
        e0, e1, e2 = e0 * (dp_own[h, 0] - delta0), e1 * (dp_own[h, 1] - delta1), e2 * (dp_own[h, 2] - delta1)
        blocks = [
            x0.astype(BF16),
            jnp.concatenate([x1, x2], axis=1).astype(BF16),
            jnp.concatenate([e0, e1], axis=1).astype(BF16),
            e2.astype(BF16),
        ]
        spans = [low, slice(0, rows), slice(0, rows), high]
        d_k = [dot(block, qn[h, span, :], (1, 0)) for block, span in zip(blocks, spans)]
        product = None
        for i, part in enumerate(d_k):
            term = part * kn[h, i * half : (i + 1) * half, :].astype(F32)
            product = term if product is None else product + term
        mass = mass + jnp.sum(product, axis=0, keepdims=True)
        same, before = e0 + e2, x1 + e1
        fold_p = fold(jnp.where(upper, same, before), lead)
        fold_n = fold(jnp.where(upper, 0.0, same), lead)
        line_p, line_n = align(fold_p), align(fold_n)
        lane = lax.broadcasted_iota(jnp.int32, line_p.shape, 1)
        rest = -jnp.sum(jnp.sum(fold_p + fold_n, axis=0, keepdims=True), axis=1, keepdims=True)
        packed.append(jnp.where(lane < lead, line_n, line_p))
        packed.append(jnp.where(lane < lead, line_p, jnp.where(lane == lead, rest, 0.0)))
        dk_out[h, low, :] = d_k[0].astype(BF16)
        dk_out[h, high, :] = d_k[1].astype(BF16)
        dk_acc[h, low, :] = d_k[2]
        dk_acc[h, high, :] = d_k[3]
        if h < heads - 1:
            start(has_prev, [dv_back[h], dk_back[h]])
        else:
            mass = mass * factor
            line_src[...] = mass
            one_src[...] = jnp.concatenate(
                packed + [mass, jnp.zeros((8 - 1 - len(packed), HEAD_DIM), F32)], axis=0
            )
            two[sp] = one_src[...]

            def spread(i):
                at = jnp.where(i >= sp, i + 1, i)
                pltpu.make_async_remote_copy(
                    src_ref=one_src, dst_ref=two.at[sp], send_sem=red_sem.at[0], recv_sem=red_sem.at[1],
                    device_id=(at, tp), device_id_type=MESH,
                ).start()

            def spread_line(at):
                for other in range(1, n_tp):
                    pltpu.make_async_remote_copy(
                        src_ref=line_src, dst_ref=lines.at[other - 1, sp], send_sem=red_sem.at[2],
                        recv_sem=red_sem.at[3], device_id=(at, lax.rem(tp + other, n_tp)), device_id_type=MESH,
                    ).start()

            def publish():
                for late in range(step, len(rounds)):
                    relay(late)
                if n_sp <= 32:
                    for i in range(n_sp - 1):
                        spread(i)
                        spread_line(i)
                    spread_line(n_sp - 1)
                else:
                    @pl.loop(0, n_sp - 1)
                    def _(i):
                        spread(i)

                    @pl.loop(0, n_sp)
                    def _(i):
                        spread_line(i)

            @pl.when(jnp.logical_not(eager))
            def _():
                publish()

            start(has_prev & jnp.logical_not(yields), [dk_back[h]])
        for i, part in enumerate([
            dot(jnp.concatenate([blocks[0], blocks[1][:, low], blocks[2][:, low]], axis=0), kn[h, 0 : 3 * half, :], (0, 0)),
            dot(jnp.concatenate([blocks[1][:, high], blocks[2][:, high], blocks[3]], axis=0), kn[h, half:, :], (0, 0)),
        ]):
            span = slice(i * half, (i + 1) * half)
            grad = part * factor * g0
            unit = q_unit[h, span, :]
            out = q_rms[h, span, :] * (grad - unit * jnp.mean(grad * unit, axis=-1, keepdims=True))
            dq_ref[span, h * HEAD_DIM : (h + 1) * HEAD_DIM] = out.astype(BF16)

    @pl.when(eager)
    def _():
        publish()

    held = [dk_back[heads - 1], dv_back[heads - 1]]

    def add_dv(h):
        @pl.when(has_next)
        def _():
            dv_acc[h] += dv_in[h].astype(F32)

        dv_ref[:, h * HEAD_DIM : (h + 1) * HEAD_DIM] = dv_acc[h].astype(BF16)

    for h in range(heads):
        across = slice(h * HEAD_DIM, (h + 1) * HEAD_DIM)

        @pl.when(has_next)
        def _():
            (dv_back if h < heads - 1 else dk_back)[h].wait_recv()

        if h == 0:
            start(has_prev & yields & jnp.logical_not(eager), held)
        if h < heads - 1:
            add_dv(h)

            @pl.when(has_next)
            def _():
                dk_back[h].wait_recv()

        if h == 0:
            start(has_prev & yields & eager, held)

        @pl.when(has_next)
        def _():
            dk_acc[h] += dk_in[h].astype(F32)

        unit = k_unit[h]
        grad = dk_acc[h] * factor * g1
        out = k_rms[h] * (grad - unit * jnp.mean(grad * unit, axis=-1, keepdims=True))
        dk_ref[:, across] = out.astype(BF16)

    peers = two.at[pl.ds(0, n_sp - 1)]
    drain(peers, red_sem.at[1])
    drain(lines, red_sem.at[3])
    whole = jnp.sum(two[...], axis=0)
    for h in range(heads):
        dt_ref[h : h + 1, 0:half] = whole[2 * h : 2 * h + 1]
        dt_ref[h : h + 1, half:] = whole[2 * h + 1 : 2 * h + 2, 0 : entries - half]
    mass = whole[2 * heads : 2 * heads + 1] + jnp.sum(lines[...], axis=(0, 1))
    dg_ref[...] = mass * inverse

    drain(peers, red_sem.at[0])
    drain(lines, red_sem.at[2])

    @pl.when(has_prev)
    def _():
        drain(out_ref, send_sem.at[1])

    @pl.when(has_next)
    def _():
        drain(kv_ref, send_sem.at[0])
        dv_back[heads - 1].wait_recv()

    add_dv(heads - 1)


def emit(*refs):
    sem = refs[-1]
    count = len(refs) // 2
    copies = [pltpu.make_async_copy(refs[i], refs[count + i], sem.at[i]) for i in range(count)]
    for copy in copies:
        copy.start()
    for copy in copies:
        copy.wait()


def solution(mesh):
    n_sp, n_tp = mesh.shape["sp"], mesh.shape["tp"]

    def local(queries, keys, values, gains, bias_table, d_out):
        rows, width = queries.shape
        heads = width // HEAD_DIM
        half = rows // 2
        assert n_sp > 1 and rows == LEFT * SEG and half == MAX_REL == HEAD_DIM and 2 * heads + 1 <= 8
        act = jax.ShapeDtypeStruct((rows, width), BF16)
        vmem = pl.BlockSpec(memory_space=pltpu.VMEM)
        shapes = (
            act, act, act,
            jax.ShapeDtypeStruct(bias_table.shape[::-1], F32),
            jax.ShapeDtypeStruct(gains.shape, F32),
        )
        low = pltpu.VMEM((heads, rows, HEAD_DIM), BF16)
        pair = pltpu.VMEM((2 * heads, rows, HEAD_DIM), BF16)
        wide = pltpu.VMEM((heads, rows, HEAD_DIM), F32)
        thin = pltpu.VMEM((heads, rows, 1), F32)
        parts = pl.pallas_call(
            functools.partial(kernel, n_sp, n_tp),
            out_shape=shapes,
            in_specs=[pl.BlockSpec(memory_space=pltpu.HBM)] * 6,
            out_specs=(vmem,) * 5,
            scratch_shapes=[
                pair, pair,
                pltpu.VMEM(gains.shape, F32),
                pltpu.VMEM(bias_table.shape[::-1], F32),
                low, low,
                pltpu.VMEM((heads, 2 * rows, HEAD_DIM), BF16),
                low,
                wide, thin, wide, thin,
                pltpu.VMEM((heads, 5, half, half), F32),
                pltpu.VMEM((heads, 3, half, half), F32),
                pltpu.VMEM((heads, 3, half, half), F32),
                wide, wide,
                pair, low, low,
                pltpu.VMEM((8, HEAD_DIM), F32),
                pltpu.VMEM((n_sp, 8, HEAD_DIM), F32),
                pltpu.VMEM((1, HEAD_DIM), F32),
                pltpu.VMEM((n_tp - 1, n_sp, 1, HEAD_DIM), F32),
                pltpu.SemaphoreType.DMA((4,)),
                pltpu.SemaphoreType.DMA((2,)),
                pltpu.SemaphoreType.DMA((4 * heads,)),
                pltpu.SemaphoreType.DMA((4,)),
                pltpu.SemaphoreType.REGULAR((max(1, (n_sp - 1).bit_length()),)),
            ],
            compiler_params=pltpu.CompilerParams(
                collective_id=0, has_side_effects=True, vmem_limit_bytes=24 * 1024 * 1024
            ),
        )(*(
            pltpu.with_memory_space_constraint(x, pltpu.HBM)
            for x in (queries, keys, values, d_out, gains, bias_table.T)
        ))
        d_q, d_k, d_v, d_table, d_gains = pl.pallas_call(
            emit,
            out_shape=shapes,
            in_specs=[vmem] * 5,
            out_specs=(pl.BlockSpec(memory_space=pltpu.HBM),) * 5,
            scratch_shapes=[pltpu.SemaphoreType.DMA((5,))],
            compiler_params=pltpu.CompilerParams(vmem_limit_bytes=8 * 1024 * 1024),
        )(*parts)
        return d_q, d_k, d_v, d_table.T, d_gains

    in_specs = (P("sp", "tp"), P("sp", "tp"), P("sp", "tp"), P(), P(None, "tp"), P("sp", "tp"))
    out_specs = (P("sp", "tp"), P("sp", "tp"), P("sp", "tp"), P(None, "tp"), P())
    return jax.shard_map(local, mesh=mesh, in_specs=in_specs, out_specs=out_specs, check_vma=False)
```

```python
import functools

import jax
import jax.numpy as jnp
from jax import lax
from jax.experimental import pallas as pl
from jax.experimental.pallas import tpu as pltpu
from jax.sharding import PartitionSpec as P

HEAD_DIM = 128
SEG = 64
LEFT = 4
MAX_REL = 128
EPSILON = 1e-06
NEG = -1e30
LOG2E = 1.4426950408889634
MESH = pl.DeviceIdType.MESH
F32 = jnp.float32
BF16 = jnp.bfloat16


def dot(a, b, contract):
    return lax.dot_general(a, b, ((contract[:1], contract[1:]), ((), ())), preferred_element_type=F32)


def unit_of(block):
    wide = block.astype(F32)
    rms = lax.rsqrt(jnp.mean(wide * wide, axis=-1, keepdims=True) + EPSILON)
    return wide * rms, rms


def fold(tile, lead):
    total = None
    for start in range(0, tile.shape[0], 8):
        turned = pltpu.roll(tile[start : start + 8], (lead - start) % tile.shape[1], 1)
        total = turned if total is None else total + turned
    return total


def align(total):
    lanes = total.shape[1]
    sublane = lax.broadcasted_iota(jnp.int32, total.shape, 0)
    line = jnp.where(sublane == 0, total, 0.0)
    for i in range(1, 8):
        line = line + jnp.where(sublane == i, pltpu.roll(total, lanes - i, 1), 0.0)
    return jnp.sum(line, axis=0, keepdims=True)


def kernel(
    n_sp, n_tp,
    q_hbm, k_hbm, v_hbm, do_hbm, g_hbm, t_hbm,
    dq_ref, dk_ref, dv_ref, dt_ref, dg_ref,
    kv_ref, qd_ref, g_ref, t_ref, k_raw, v_prev, kn, qn, q_unit, q_rms, k_unit, k_rms,
    tiles, e_own, dp_own, dk_acc, dv_acc, out_ref, dk_in, dv_in, one_src, two, line_src, lines,
    load_sem, send_sem, recv_sem, red_sem, hand_sem,
):
    heads, rows, _ = k_raw.shape
    k_ref, v_ref = kv_ref.at[pl.ds(0, heads)], kv_ref.at[pl.ds(heads, heads)]
    q_ref, do_ref = qd_ref.at[pl.ds(0, heads)], qd_ref.at[pl.ds(heads, heads)]
    dk_out, dv_out = out_ref.at[pl.ds(0, heads)], out_ref.at[pl.ds(heads, heads)]
    half = rows // 2
    entries = t_ref.shape[1]
    lead = SEG - 1
    factor = HEAD_DIM ** (-0.5)
    scale = factor * LOG2E
    sp, tp = lax.axis_index("sp"), lax.axis_index("tp")
    has_prev, has_next = sp > 0, sp < n_sp - 1
    nxt, prv = sp + 1, sp - 1

    def load(src, dst, slot):
        return pltpu.make_async_copy(src, dst, load_sem.at[slot])

    def by_head(src, dst, slot):
        return [load(src.at[:, pl.ds(h * HEAD_DIM, HEAD_DIM)], dst.at[h], slot) for h in range(heads)]

    def drain(ref, sem):
        pltpu.make_async_copy(ref, ref, sem).wait()

    def signal(sem, at, core):
        pl.semaphore_signal(sem, inc=1, device_id=(at, core), device_id_type=MESH)

    def around(sem, radius):
        @pl.when(sp >= radius)
        def _():
            signal(sem, sp - radius, tp)

        @pl.when(sp < n_sp - radius)
        def _():
            signal(sem, sp + radius, tp)

    def count_around(radius):
        return jnp.where(sp >= radius, 1, 0) + jnp.where(sp < n_sp - radius, 1, 0)

    barrier = pltpu.get_barrier_semaphore()
    around(barrier, 1)
    for other in range(1, n_tp):
        signal(barrier, sp, lax.rem(tp + other, n_tp))
    load_small = [load(t_hbm, t_ref, 2), load(g_hbm, g_ref, 3)]
    for copy in (
        by_head(k_hbm, k_ref, 0) + by_head(v_hbm, v_ref, 0) + load_small
        + by_head(q_hbm, q_ref, 1) + by_head(do_hbm, do_ref, 1)
    ):
        copy.start()

    pl.semaphore_wait(barrier, count_around(1) + n_tp - 1)

    rounds = []
    while 2 ** len(rounds) < n_sp:
        rounds.append(2 ** len(rounds))

    def say(step):
        around(hand_sem.at[step], rounds[step])

    def hear(step):
        pl.semaphore_wait(hand_sem.at[step], count_around(rounds[step]))

    def send(slot, src, dst, to):
        return pltpu.make_async_remote_copy(
            src_ref=src, dst_ref=dst, send_sem=send_sem.at[slot % 4 // 2], recv_sem=recv_sem.at[slot],
            device_id=(to, tp), device_id_type=MESH,
        )

    k_next = [send(4 * h, k_ref.at[h], k_raw.at[h], nxt) for h in range(heads)]
    v_next = [send(4 * h + 1, v_ref.at[h], v_prev.at[h], nxt) for h in range(heads)]
    dv_back = [send(4 * h + 2, dv_out.at[h], dv_in.at[h], prv) for h in range(heads)]
    dk_back = [send(4 * h + 3, dk_out.at[h], dk_in.at[h], prv) for h in range(heads)]

    def start(gate, copies):
        @pl.when(gate)
        def _():
            for copy in copies:
                copy.start()

    drain(kv_ref, load_sem.at[0])
    yields = tp == n_tp - 1
    eager = sp < n_sp // 4
    start(has_next, [k_next[0], v_next[0]])
    start(has_next & jnp.logical_not(yields), k_next[1:] + v_next[1:])
    say(0)
    for copy in load_small:
        copy.wait()

    @pl.when(jnp.logical_not(has_prev))
    def _():
        kn[:, 0:rows, :] = jnp.zeros((heads, rows, HEAD_DIM), BF16)
        v_prev[...] = jnp.zeros((heads, rows, HEAD_DIM), BF16)

    g0, g1 = g_ref[0:1, :], g_ref[1:2, :]
    low, high = slice(0, half), slice(half, rows)
    row = lax.broadcasted_iota(jnp.int32, (half, half), 0)
    col = lax.broadcasted_iota(jnp.int32, (half, half), 1)
    upper = col >= row
    absent = jnp.where(has_prev, 0.0, NEG)

    table = jnp.concatenate([t_ref[...], jnp.zeros((heads, 2 * half - entries), F32)], axis=1)
    table = pltpu.roll(table, 2 * half - lead, 1)
    for h in range(heads):
        def skew(line):
            return pltpu.roll(jnp.broadcast_to(line, (half, half)), 0, 1, stride=1, stride_axis=0)

        close = skew(table[h : h + 1, 0:half])
        ahead = skew(table[h : h + 1, half:])
        far = jnp.broadcast_to(table[h : h + 1, half : half + 1], (half, half))
        same = jnp.where(upper, close, ahead)
        same = jnp.where((row >= SEG) & (col < SEG), NEG, same)
        before = jnp.where(upper, far, close)
        distant = jnp.where((row < SEG) & (col >= SEG), NEG, far)
        top_own = jnp.max(same, axis=0, keepdims=True)
        top = jnp.maximum(top_own, jnp.max(before, axis=0, keepdims=True))
        first_top = jnp.where(has_prev, top, top_own)
        tiles[h, 0] = (same - first_top) * LOG2E
        tiles[h, 1] = (before - top) * LOG2E
        tiles[h, 2] = (same - top) * LOG2E
        tiles[h, 3] = (distant - top) * LOG2E + absent
        tiles[h, 4] = (before - top) * LOG2E + absent

    inverse = 1.0 / g_ref[...]
    for h in range(heads):
        unit, rms = unit_of(k_ref[h])
        k_unit[h] = unit
        k_rms[h] = rms
        kn[h, rows:, :] = (unit * g1).astype(BF16)
    drain(qd_ref, load_sem.at[1])

    sums = []
    for h in range(heads):
        unit, rms = unit_of(q_ref[h])
        q_unit[h] = unit
        q_rms[h] = rms
        qn[h] = (unit * g0).astype(BF16)
        s0 = dot(kn[h, rows : rows + half, :], qn[h], (1, 1)) * scale
        s1 = dot(kn[h, rows + half :, :], qn[h, high, :], (1, 1)) * scale
        e0 = jnp.exp2(s0[:, low] + tiles[h, 0])
        e1 = jnp.exp2(s0[:, high] + tiles[h, 1])
        e2 = jnp.exp2(s1 + tiles[h, 2])
        e_own[h, 0], e_own[h, 1], e_own[h, 2] = e0, e1, e2
        p0 = dot(v_ref[h, low, :], do_ref[h], (1, 1))
        dp_own[h, 0], dp_own[h, 1] = p0[:, low], p0[:, high]
        dp_own[h, 2] = dot(v_ref[h, high, :], do_ref[h, high, :], (1, 1))
        sums.append((
            jnp.sum(e0, axis=0, keepdims=True),
            jnp.sum(e1, axis=0, keepdims=True) + jnp.sum(e2, axis=0, keepdims=True),
        ))
    step = 0

    def relay(step):
        if step < len(rounds):
            hear(step)
            if step + 1 < len(rounds):
                say(step + 1)
        return step + 1

    step = relay(step)
    step = relay(step)
    packed = []
    mass = jnp.zeros((1, HEAD_DIM), F32)
    for h in range(heads):
        @pl.when(has_prev)
        def _():
            k_next[h].wait_recv()
            kn[h, 0:rows, :] = (unit_of(k_raw[h])[0] * g1).astype(BF16)

        s0 = dot(kn[h, low, :], qn[h, low, :], (1, 1)) * scale
        s1 = dot(kn[h, high, :], qn[h], (1, 1)) * scale
        x0 = jnp.exp2(s0 + tiles[h, 3])
        x1 = jnp.exp2(s1[:, low] + tiles[h, 4])
        x2 = jnp.exp2(s1[:, high] + tiles[h, 3])
        r0 = 1.0 / (sums[h][0] + jnp.sum(x0 + x1, axis=0, keepdims=True))
        r1 = 1.0 / (sums[h][1] + jnp.sum(x2, axis=0, keepdims=True))
        x0, x1, x2 = x0 * r0, x1 * r0, x2 * r1
        e0, e1, e2 = e_own[h, 0] * r0, e_own[h, 1] * r1, e_own[h, 2] * r1
        d_o = do_ref[h]
        dv_out[h, low, :] = dot(x0.astype(BF16), d_o[low], (1, 0)).astype(BF16)
        dv_out[h, high, :] = dot(jnp.concatenate([x1, x2], axis=1).astype(BF16), d_o, (1, 0)).astype(BF16)
        dv_acc[h, low, :] = dot(jnp.concatenate([e0, e1], axis=1).astype(BF16), d_o, (1, 0))
        dv_acc[h, high, :] = dot(e2.astype(BF16), d_o[high], (1, 0))
        if h == heads - 1:
            start(has_prev & jnp.logical_not(yields), [dv_back[h]])
        if step < len(rounds) - 1:
            step = relay(step)
        own0 = jnp.sum(e0 * dp_own[h, 0], axis=0, keepdims=True)
        own1 = jnp.sum(e1 * dp_own[h, 1] + e2 * dp_own[h, 2], axis=0, keepdims=True)

        @pl.when(has_prev)
        def _():
            v_next[h].wait_recv()

        if h == 0:
            start(has_next & yields, k_next[1:] + v_next[1:])
        p0 = dot(v_prev[h, low, :], d_o[low], (1, 1))
        p1 = dot(v_prev[h, high, :], d_o, (1, 1))
        delta0 = own0 + jnp.sum(x0 * p0 + x1 * p1[:, low], axis=0, keepdims=True)
        delta1 = own1 + jnp.sum(x2 * p1[:, high], axis=0, keepdims=True)
        x0, x1, x2 = x0 * (p0 - delta0), x1 * (p1[:, low] - delta0), x2 * (p1[:, high] - delta1)
        e0, e1, e2 = e0 * (dp_own[h, 0] - delta0), e1 * (dp_own[h, 1] - delta1), e2 * (dp_own[h, 2] - delta1)
        blocks = [
            x0.astype(BF16),
            jnp.concatenate([x1, x2], axis=1).astype(BF16),
            jnp.concatenate([e0, e1], axis=1).astype(BF16),
            e2.astype(BF16),
        ]
        spans = [low, slice(0, rows), slice(0, rows), high]
        d_k = [dot(block, qn[h, span, :], (1, 0)) for block, span in zip(blocks, spans)]
        product = None
        for i, part in enumerate(d_k):
            term = part * kn[h, i * half : (i + 1) * half, :].astype(F32)
            product = term if product is None else product + term
        mass = mass + jnp.sum(product, axis=0, keepdims=True)
        same, before = e0 + e2, x1 + e1
        fold_p = fold(jnp.where(upper, same, before), lead)
        fold_n = fold(jnp.where(upper, 0.0, same), lead)
        line_p, line_n = align(fold_p), align(fold_n)
        lane = lax.broadcasted_iota(jnp.int32, line_p.shape, 1)
        rest = -jnp.sum(jnp.sum(fold_p + fold_n, axis=0, keepdims=True), axis=1, keepdims=True)
        packed.append(jnp.where(lane < lead, line_n, line_p))
        packed.append(jnp.where(lane < lead, line_p, jnp.where(lane == lead, rest, 0.0)))
        dk_out[h, low, :] = d_k[0].astype(BF16)
        dk_out[h, high, :] = d_k[1].astype(BF16)
        dk_acc[h, low, :] = d_k[2]
        dk_acc[h, high, :] = d_k[3]
        if h < heads - 1:
            start(has_prev, [dv_back[h], dk_back[h]])
        else:
            mass = mass * factor
            line_src[...] = mass
            one_src[...] = jnp.concatenate(
                packed + [mass, jnp.zeros((8 - 1 - len(packed), HEAD_DIM), F32)], axis=0
            )
            two[sp] = one_src[...]

            def spread(i):
                at = jnp.where(i >= sp, i + 1, i)
                pltpu.make_async_remote_copy(
                    src_ref=one_src, dst_ref=two.at[sp], send_sem=red_sem.at[0], recv_sem=red_sem.at[1],
                    device_id=(at, tp), device_id_type=MESH,
                ).start()

            def spread_line(at):
                for other in range(1, n_tp):
                    pltpu.make_async_remote_copy(
                        src_ref=line_src, dst_ref=lines.at[other - 1, sp], send_sem=red_sem.at[2],
                        recv_sem=red_sem.at[3], device_id=(at, lax.rem(tp + other, n_tp)), device_id_type=MESH,
                    ).start()

            def publish():
                for late in range(step, len(rounds)):
                    relay(late)
                if n_sp <= 32:
                    for i in range(n_sp - 1):
                        spread(i)
                        spread_line(i)
                    spread_line(n_sp - 1)
                else:
                    @pl.loop(0, n_sp - 1)
                    def _(i):
                        spread(i)

                    @pl.loop(0, n_sp)
                    def _(i):
                        spread_line(i)

            @pl.when(jnp.logical_not(eager))
            def _():
                publish()

            start(has_prev & jnp.logical_not(yields), [dk_back[h]])
        for i, part in enumerate([
            dot(jnp.concatenate([blocks[0], blocks[1][:, low], blocks[2][:, low]], axis=0), kn[h, 0 : 3 * half, :], (0, 0)),
            dot(jnp.concatenate([blocks[1][:, high], blocks[2][:, high], blocks[3]], axis=0), kn[h, half:, :], (0, 0)),
        ]):
            span = slice(i * half, (i + 1) * half)
            grad = part * factor * g0
            unit = q_unit[h, span, :]
            out = q_rms[h, span, :] * (grad - unit * jnp.mean(grad * unit, axis=-1, keepdims=True))
            dq_ref[span, h * HEAD_DIM : (h + 1) * HEAD_DIM] = out.astype(BF16)

    @pl.when(eager)
    def _():
        publish()

    held = [dk_back[heads - 1], dv_back[heads - 1]]

    def add_dv(h):
        @pl.when(has_next)
        def _():
            dv_acc[h] += dv_in[h].astype(F32)

        dv_ref[:, h * HEAD_DIM : (h + 1) * HEAD_DIM] = dv_acc[h].astype(BF16)

    for h in range(heads):
        across = slice(h * HEAD_DIM, (h + 1) * HEAD_DIM)

        @pl.when(has_next)
        def _():
            (dv_back if h < heads - 1 else dk_back)[h].wait_recv()

        if h < heads - 1:
            add_dv(h)

            @pl.when(has_next)
            def _():
                dk_back[h].wait_recv()

        if h == 0:
            start(has_prev & yields, held)

        @pl.when(has_next)
        def _():
            dk_acc[h] += dk_in[h].astype(F32)

        unit = k_unit[h]
        grad = dk_acc[h] * factor * g1
        out = k_rms[h] * (grad - unit * jnp.mean(grad * unit, axis=-1, keepdims=True))
        dk_ref[:, across] = out.astype(BF16)

    peers = two.at[pl.ds(0, n_sp - 1)]
    drain(peers, red_sem.at[1])
    drain(lines, red_sem.at[3])
    whole = jnp.sum(two[...], axis=0)
    for h in range(heads):
        dt_ref[h : h + 1, 0:half] = whole[2 * h : 2 * h + 1]
        dt_ref[h : h + 1, half:] = whole[2 * h + 1 : 2 * h + 2, 0 : entries - half]
    mass = whole[2 * heads : 2 * heads + 1] + jnp.sum(lines[...], axis=(0, 1))
    dg_ref[...] = mass * inverse

    drain(peers, red_sem.at[0])
    drain(lines, red_sem.at[2])

    @pl.when(has_prev)
    def _():
        drain(out_ref, send_sem.at[1])

    @pl.when(has_next)
    def _():
        drain(kv_ref, send_sem.at[0])
        dv_back[heads - 1].wait_recv()

    add_dv(heads - 1)


def emit(*refs):
    sem = refs[-1]
    count = len(refs) // 2
    copies = [pltpu.make_async_copy(refs[i], refs[count + i], sem.at[i]) for i in range(count)]
    for copy in copies:
        copy.start()
    for copy in copies:
        copy.wait()


def solution(mesh):
    n_sp, n_tp = mesh.shape["sp"], mesh.shape["tp"]

    def local(queries, keys, values, gains, bias_table, d_out):
        rows, width = queries.shape
        heads = width // HEAD_DIM
        half = rows // 2
        assert n_sp > 1 and rows == LEFT * SEG and half == MAX_REL == HEAD_DIM and 2 * heads + 1 <= 8
        act = jax.ShapeDtypeStruct((rows, width), BF16)
        vmem = pl.BlockSpec(memory_space=pltpu.VMEM)
        shapes = (
            act, act, act,
            jax.ShapeDtypeStruct(bias_table.shape[::-1], F32),
            jax.ShapeDtypeStruct(gains.shape, F32),
        )
        low = pltpu.VMEM((heads, rows, HEAD_DIM), BF16)
        pair = pltpu.VMEM((2 * heads, rows, HEAD_DIM), BF16)
        wide = pltpu.VMEM((heads, rows, HEAD_DIM), F32)
        thin = pltpu.VMEM((heads, rows, 1), F32)
        parts = pl.pallas_call(
            functools.partial(kernel, n_sp, n_tp),
            out_shape=shapes,
            in_specs=[pl.BlockSpec(memory_space=pltpu.HBM)] * 6,
            out_specs=(vmem,) * 5,
            scratch_shapes=[
                pair, pair,
                pltpu.VMEM(gains.shape, F32),
                pltpu.VMEM(bias_table.shape[::-1], F32),
                low, low,
                pltpu.VMEM((heads, 2 * rows, HEAD_DIM), BF16),
                low,
                wide, thin, wide, thin,
                pltpu.VMEM((heads, 5, half, half), F32),
                pltpu.VMEM((heads, 3, half, half), F32),
                pltpu.VMEM((heads, 3, half, half), F32),
                wide, wide,
                pair, low, low,
                pltpu.VMEM((8, HEAD_DIM), F32),
                pltpu.VMEM((n_sp, 8, HEAD_DIM), F32),
                pltpu.VMEM((1, HEAD_DIM), F32),
                pltpu.VMEM((n_tp - 1, n_sp, 1, HEAD_DIM), F32),
                pltpu.SemaphoreType.DMA((4,)),
                pltpu.SemaphoreType.DMA((2,)),
                pltpu.SemaphoreType.DMA((4 * heads,)),
                pltpu.SemaphoreType.DMA((4,)),
                pltpu.SemaphoreType.REGULAR((max(1, (n_sp - 1).bit_length()),)),
            ],
            compiler_params=pltpu.CompilerParams(
                collective_id=0, has_side_effects=True, vmem_limit_bytes=24 * 1024 * 1024
            ),
        )(*(
            pltpu.with_memory_space_constraint(x, pltpu.HBM)
            for x in (queries, keys, values, d_out, gains, bias_table.T)
        ))
        d_q, d_k, d_v, d_table, d_gains = pl.pallas_call(
            emit,
            out_shape=shapes,
            in_specs=[vmem] * 5,
            out_specs=(pl.BlockSpec(memory_space=pltpu.HBM),) * 5,
            scratch_shapes=[pltpu.SemaphoreType.DMA((5,))],
            compiler_params=pltpu.CompilerParams(vmem_limit_bytes=8 * 1024 * 1024),
        )(*parts)
        return d_q, d_k, d_v, d_table.T, d_gains

    in_specs = (P("sp", "tp"), P("sp", "tp"), P("sp", "tp"), P(), P(None, "tp"), P("sp", "tp"))
    out_specs = (P("sp", "tp"), P("sp", "tp"), P("sp", "tp"), P(None, "tp"), P())
    return jax.shard_map(local, mesh=mesh, in_specs=in_specs, out_specs=out_specs, check_vma=False)
```

```python
import functools

import jax
import jax.numpy as jnp
from jax import lax
from jax.experimental import pallas as pl
from jax.experimental.pallas import tpu as pltpu
from jax.sharding import PartitionSpec as P

HEAD_DIM = 128
SEG = 64
LEFT = 4
MAX_REL = 128
EPSILON = 1e-06
NEG = -1e30
LOG2E = 1.4426950408889634
MESH = pl.DeviceIdType.MESH
F32 = jnp.float32
BF16 = jnp.bfloat16


def dot(a, b, contract):
    return lax.dot_general(a, b, ((contract[:1], contract[1:]), ((), ())), preferred_element_type=F32)


def unit_of(block):
    wide = block.astype(F32)
    rms = lax.rsqrt(jnp.mean(wide * wide, axis=-1, keepdims=True) + EPSILON)
    return wide * rms, rms


def fold(tile, lead):
    total = None
    for start in range(0, tile.shape[0], 8):
        turned = pltpu.roll(tile[start : start + 8], (lead - start) % tile.shape[1], 1)
        total = turned if total is None else total + turned
    return total


def align(total):
    lanes = total.shape[1]
    sublane = lax.broadcasted_iota(jnp.int32, total.shape, 0)
    line = jnp.where(sublane == 0, total, 0.0)
    for i in range(1, 8):
        line = line + jnp.where(sublane == i, pltpu.roll(total, lanes - i, 1), 0.0)
    return jnp.sum(line, axis=0, keepdims=True)


def kernel(
    n_sp, n_tp,
    q_hbm, k_hbm, v_hbm, do_hbm, g_hbm, t_hbm,
    dq_ref, dk_ref, dv_ref, dt_ref, dg_ref,
    kv_ref, qd_ref, g_ref, t_ref, k_raw, v_prev, kn, qn, q_unit, q_rms, k_unit, k_rms,
    tiles, e_own, dp_own, dk_acc, dv_acc, out_ref, dk_in, dv_in, one_src, two, line_src, lines,
    load_sem, recv_sem, red_sem, hand_sem,
):
    heads, rows, _ = k_raw.shape
    k_ref, v_ref = kv_ref.at[pl.ds(0, heads)], kv_ref.at[pl.ds(heads, heads)]
    q_ref, do_ref = qd_ref.at[pl.ds(0, heads)], qd_ref.at[pl.ds(heads, heads)]
    dk_out, dv_out = out_ref.at[pl.ds(0, heads)], out_ref.at[pl.ds(heads, heads)]
    half = rows // 2
    entries = t_ref.shape[1]
    lead = SEG - 1
    factor = HEAD_DIM ** (-0.5)
    scale = factor * LOG2E
    sp, tp = lax.axis_index("sp"), lax.axis_index("tp")
    has_prev, has_next = sp > 0, sp < n_sp - 1
    nxt, prv = sp + 1, sp - 1

    def load(src, dst, slot):
        return pltpu.make_async_copy(src, dst, load_sem.at[slot])

    def by_head(src, dst, slot):
        return [load(src.at[:, pl.ds(h * HEAD_DIM, HEAD_DIM)], dst.at[h], slot) for h in range(heads)]

    def drain(ref, sem):
        pltpu.make_async_copy(ref, ref, sem).wait()

    def signal(sem, at, core):
        pl.semaphore_signal(sem, inc=1, device_id=(at, core), device_id_type=MESH)

    def around(sem, radius):
        @pl.when(sp >= radius)
        def _():
            signal(sem, sp - radius, tp)

        @pl.when(sp < n_sp - radius)
        def _():
            signal(sem, sp + radius, tp)

    def count_around(radius):
        return jnp.where(sp >= radius, 1, 0) + jnp.where(sp < n_sp - radius, 1, 0)

    barrier = pltpu.get_barrier_semaphore()
    around(barrier, 1)
    for other in range(1, n_tp):
        signal(barrier, sp, lax.rem(tp + other, n_tp))
    load_small = [load(t_hbm, t_ref, 2), load(g_hbm, g_ref, 3)]
    for copy in (
        by_head(k_hbm, k_ref, 0) + by_head(v_hbm, v_ref, 0) + load_small
        + by_head(q_hbm, q_ref, 1) + by_head(do_hbm, do_ref, 1)
    ):
        copy.start()

    pl.semaphore_wait(barrier, count_around(1) + n_tp - 1)

    rounds = []
    while 2 ** len(rounds) < n_sp:
        rounds.append(2 ** len(rounds))

    def say(step):
        around(hand_sem.at[step], rounds[step])

    def hear(step):
        pl.semaphore_wait(hand_sem.at[step], count_around(rounds[step]))

    def send(slot, src, dst, to):
        return pltpu.make_async_remote_copy(
            src_ref=src, dst_ref=dst, send_sem=load_sem.at[slot % 4 // 2], recv_sem=recv_sem.at[slot],
            device_id=(to, tp), device_id_type=MESH,
        )

    k_next = [send(4 * h, k_ref.at[h], k_raw.at[h], nxt) for h in range(heads)]
    v_next = [send(4 * h + 1, v_ref.at[h], v_prev.at[h], nxt) for h in range(heads)]
    dv_back = [send(4 * h + 2, dv_out.at[h], dv_in.at[h], prv) for h in range(heads)]
    dk_back = [send(4 * h + 3, dk_out.at[h], dk_in.at[h], prv) for h in range(heads)]

    def start(gate, copies):
        @pl.when(gate)
        def _():
            for copy in copies:
                copy.start()

    drain(kv_ref, load_sem.at[0])
    yields = tp == n_tp - 1
    eager = sp < n_sp // 4
    start(has_next, [k_next[0], v_next[0]])
    start(has_next & jnp.logical_not(yields), k_next[1:] + v_next[1:])
    say(0)
    for copy in load_small:
        copy.wait()

    @pl.when(jnp.logical_not(has_prev))
    def _():
        kn[:, 0:rows, :] = jnp.zeros((heads, rows, HEAD_DIM), BF16)
        v_prev[...] = jnp.zeros((heads, rows, HEAD_DIM), BF16)

    g0, g1 = g_ref[0:1, :], g_ref[1:2, :]
    low, high = slice(0, half), slice(half, rows)
    row = lax.broadcasted_iota(jnp.int32, (half, half), 0)
    col = lax.broadcasted_iota(jnp.int32, (half, half), 1)
    upper = col >= row
    absent = jnp.where(has_prev, 0.0, NEG)

    table = jnp.concatenate([t_ref[...], jnp.zeros((heads, 2 * half - entries), F32)], axis=1)
    table = pltpu.roll(table, 2 * half - lead, 1)
    for h in range(heads):
        def skew(line):
            return pltpu.roll(jnp.broadcast_to(line, (half, half)), 0, 1, stride=1, stride_axis=0)

        close = skew(table[h : h + 1, 0:half])
        ahead = skew(table[h : h + 1, half:])
        far = jnp.broadcast_to(table[h : h + 1, half : half + 1], (half, half))
        same = jnp.where(upper, close, ahead)
        same = jnp.where((row >= SEG) & (col < SEG), NEG, same)
        before = jnp.where(upper, far, close)
        distant = jnp.where((row < SEG) & (col >= SEG), NEG, far)
        top_own = jnp.max(same, axis=0, keepdims=True)
        top = jnp.maximum(top_own, jnp.max(before, axis=0, keepdims=True))
        first_top = jnp.where(has_prev, top, top_own)
        tiles[h, 0] = (same - first_top) * LOG2E
        tiles[h, 1] = (before - top) * LOG2E
        tiles[h, 2] = (same - top) * LOG2E
        tiles[h, 3] = (distant - top) * LOG2E + absent
        tiles[h, 4] = (before - top) * LOG2E + absent

    inverse = 1.0 / g_ref[...]
    for h in range(heads):
        unit, rms = unit_of(k_ref[h])
        k_unit[h] = unit
        k_rms[h] = rms
        kn[h, rows:, :] = (unit * g1).astype(BF16)
    drain(qd_ref, load_sem.at[1])

    sums = []
    for h in range(heads):
        unit, rms = unit_of(q_ref[h])
        q_unit[h] = unit
        q_rms[h] = rms
        qn[h] = (unit * g0).astype(BF16)
        s0 = dot(kn[h, rows : rows + half, :], qn[h], (1, 1)) * scale
        s1 = dot(kn[h, rows + half :, :], qn[h, high, :], (1, 1)) * scale
        e0 = jnp.exp2(s0[:, low] + tiles[h, 0])
        e1 = jnp.exp2(s0[:, high] + tiles[h, 1])
        e2 = jnp.exp2(s1 + tiles[h, 2])
        e_own[h, 0], e_own[h, 1], e_own[h, 2] = e0, e1, e2
        p0 = dot(v_ref[h, low, :], do_ref[h], (1, 1))
        dp_own[h, 0], dp_own[h, 1] = p0[:, low], p0[:, high]
        dp_own[h, 2] = dot(v_ref[h, high, :], do_ref[h, high, :], (1, 1))
        sums.append((
            jnp.sum(e0, axis=0, keepdims=True),
            jnp.sum(e1, axis=0, keepdims=True) + jnp.sum(e2, axis=0, keepdims=True),
        ))
    step = 0

    def relay(step):
        if step < len(rounds):
            hear(step)
            if step + 1 < len(rounds):
                say(step + 1)
        return step + 1

    step = relay(step)
    step = relay(step)
    packed = []
    mass = jnp.zeros((1, HEAD_DIM), F32)
    for h in range(heads):
        @pl.when(has_prev)
        def _():
            k_next[h].wait_recv()
            kn[h, 0:rows, :] = (unit_of(k_raw[h])[0] * g1).astype(BF16)

        s0 = dot(kn[h, low, :], qn[h, low, :], (1, 1)) * scale
        s1 = dot(kn[h, high, :], qn[h], (1, 1)) * scale
        x0 = jnp.exp2(s0 + tiles[h, 3])
        x1 = jnp.exp2(s1[:, low] + tiles[h, 4])
        x2 = jnp.exp2(s1[:, high] + tiles[h, 3])
        r0 = 1.0 / (sums[h][0] + jnp.sum(x0 + x1, axis=0, keepdims=True))
        r1 = 1.0 / (sums[h][1] + jnp.sum(x2, axis=0, keepdims=True))
        x0, x1, x2 = x0 * r0, x1 * r0, x2 * r1
        e0, e1, e2 = e_own[h, 0] * r0, e_own[h, 1] * r1, e_own[h, 2] * r1
        d_o = do_ref[h]
        dv_out[h, low, :] = dot(x0.astype(BF16), d_o[low], (1, 0)).astype(BF16)
        dv_out[h, high, :] = dot(jnp.concatenate([x1, x2], axis=1).astype(BF16), d_o, (1, 0)).astype(BF16)
        dv_acc[h, low, :] = dot(jnp.concatenate([e0, e1], axis=1).astype(BF16), d_o, (1, 0))
        dv_acc[h, high, :] = dot(e2.astype(BF16), d_o[high], (1, 0))
        if h == heads - 1:
            start(has_prev & jnp.logical_not(yields), [dv_back[h]])
        if step < len(rounds) - 1:
            step = relay(step)
        own0 = jnp.sum(e0 * dp_own[h, 0], axis=0, keepdims=True)
        own1 = jnp.sum(e1 * dp_own[h, 1] + e2 * dp_own[h, 2], axis=0, keepdims=True)

        @pl.when(has_prev)
        def _():
            v_next[h].wait_recv()

        if h == 0:
            start(has_next & yields, k_next[1:] + v_next[1:])
        p0 = dot(v_prev[h, low, :], d_o[low], (1, 1))
        p1 = dot(v_prev[h, high, :], d_o, (1, 1))
        delta0 = own0 + jnp.sum(x0 * p0 + x1 * p1[:, low], axis=0, keepdims=True)
        delta1 = own1 + jnp.sum(x2 * p1[:, high], axis=0, keepdims=True)
        x0, x1, x2 = x0 * (p0 - delta0), x1 * (p1[:, low] - delta0), x2 * (p1[:, high] - delta1)
        e0, e1, e2 = e0 * (dp_own[h, 0] - delta0), e1 * (dp_own[h, 1] - delta1), e2 * (dp_own[h, 2] - delta1)
        blocks = [
            x0.astype(BF16),
            jnp.concatenate([x1, x2], axis=1).astype(BF16),
            jnp.concatenate([e0, e1], axis=1).astype(BF16),
            e2.astype(BF16),
        ]
        spans = [low, slice(0, rows), slice(0, rows), high]
        d_k = [dot(block, qn[h, span, :], (1, 0)) for block, span in zip(blocks, spans)]
        product = None
        for i, part in enumerate(d_k):
            term = part * kn[h, i * half : (i + 1) * half, :].astype(F32)
            product = term if product is None else product + term
        mass = mass + jnp.sum(product, axis=0, keepdims=True)
        same, before = e0 + e2, x1 + e1
        fold_p = fold(jnp.where(upper, same, before), lead)
        fold_n = fold(jnp.where(upper, 0.0, same), lead)
        line_p, line_n = align(fold_p), align(fold_n)
        lane = lax.broadcasted_iota(jnp.int32, line_p.shape, 1)
        rest = -jnp.sum(jnp.sum(fold_p + fold_n, axis=0, keepdims=True), axis=1, keepdims=True)
        packed.append(jnp.where(lane < lead, line_n, line_p))
        packed.append(jnp.where(lane < lead, line_p, jnp.where(lane == lead, rest, 0.0)))
        dk_out[h, low, :] = d_k[0].astype(BF16)
        dk_out[h, high, :] = d_k[1].astype(BF16)
        dk_acc[h, low, :] = d_k[2]
        dk_acc[h, high, :] = d_k[3]
        if h < heads - 1:
            start(has_prev, [dv_back[h], dk_back[h]])
        else:
            mass = mass * factor
            line_src[...] = mass
            one_src[...] = jnp.concatenate(
                packed + [mass, jnp.zeros((8 - 1 - len(packed), HEAD_DIM), F32)], axis=0
            )
            two[sp] = one_src[...]

            def spread(i):
                at = jnp.where(i >= sp, i + 1, i)
                pltpu.make_async_remote_copy(
                    src_ref=one_src, dst_ref=two.at[sp], send_sem=load_sem.at[2], recv_sem=red_sem.at[0],
                    device_id=(at, tp), device_id_type=MESH,
                ).start()

            def spread_line(at):
                for other in range(1, n_tp):
                    pltpu.make_async_remote_copy(
                        src_ref=line_src, dst_ref=lines.at[other - 1, sp], send_sem=load_sem.at[3],
                        recv_sem=red_sem.at[1], device_id=(at, lax.rem(tp + other, n_tp)), device_id_type=MESH,
                    ).start()

            def publish():
                for late in range(step, len(rounds)):
                    relay(late)
                if n_sp <= 32:
                    for i in range(n_sp - 1):
                        spread(i)
                        spread_line(i)
                    spread_line(n_sp - 1)
                else:
                    @pl.loop(0, n_sp - 1)
                    def _(i):
                        spread(i)

                    @pl.loop(0, n_sp)
                    def _(i):
                        spread_line(i)

            @pl.when(jnp.logical_not(eager))
            def _():
                publish()

            start(has_prev & jnp.logical_not(yields), [dk_back[h]])
        for i, part in enumerate([
            dot(jnp.concatenate([blocks[0], blocks[1][:, low], blocks[2][:, low]], axis=0), kn[h, 0 : 3 * half, :], (0, 0)),
            dot(jnp.concatenate([blocks[1][:, high], blocks[2][:, high], blocks[3]], axis=0), kn[h, half:, :], (0, 0)),
        ]):
            span = slice(i * half, (i + 1) * half)
            grad = part * factor * g0
            unit = q_unit[h, span, :]
            out = q_rms[h, span, :] * (grad - unit * jnp.mean(grad * unit, axis=-1, keepdims=True))
            dq_ref[span, h * HEAD_DIM : (h + 1) * HEAD_DIM] = out.astype(BF16)

    @pl.when(eager)
    def _():
        publish()

    held = [dk_back[heads - 1], dv_back[heads - 1]]

    def add_dv(h):
        @pl.when(has_next)
        def _():
            dv_acc[h] += dv_in[h].astype(F32)

        dv_ref[:, h * HEAD_DIM : (h + 1) * HEAD_DIM] = dv_acc[h].astype(BF16)

    def finish_dv():
        @pl.when(has_next)
        def _():
            dv_back[heads - 1].wait_recv()

        add_dv(heads - 1)

    for h in range(heads):
        across = slice(h * HEAD_DIM, (h + 1) * HEAD_DIM)

        if h == heads - 1:
            @pl.when(jnp.logical_not(yields))
            def _():
                finish_dv()

        @pl.when(has_next)
        def _():
            (dv_back if h < heads - 1 else dk_back)[h].wait_recv()

        if h < heads - 1:
            add_dv(h)

            @pl.when(has_next)
            def _():
                dk_back[h].wait_recv()

        if h == 0:
            start(has_prev & yields, held)

        @pl.when(has_next)
        def _():
            dk_acc[h] += dk_in[h].astype(F32)

        unit = k_unit[h]
        grad = dk_acc[h] * factor * g1
        out = k_rms[h] * (grad - unit * jnp.mean(grad * unit, axis=-1, keepdims=True))
        dk_ref[:, across] = out.astype(BF16)

    peers = two.at[pl.ds(0, n_sp - 1)]
    drain(peers, red_sem.at[0])
    drain(lines, red_sem.at[1])
    whole = jnp.sum(two[...], axis=0)
    for h in range(heads):
        dt_ref[h : h + 1, 0:half] = whole[2 * h : 2 * h + 1]
        dt_ref[h : h + 1, half:] = whole[2 * h + 1 : 2 * h + 2, 0 : entries - half]
    mass = whole[2 * heads : 2 * heads + 1] + jnp.sum(lines[...], axis=(0, 1))
    dg_ref[...] = mass * inverse

    drain(peers, load_sem.at[2])
    drain(lines, load_sem.at[3])

    @pl.when(has_prev)
    def _():
        drain(out_ref, load_sem.at[1])

    @pl.when(has_next)
    def _():
        drain(kv_ref, load_sem.at[0])

    @pl.when(yields)
    def _():
        finish_dv()


def emit(*refs):
    sem = refs[-1]
    count = len(refs) // 2
    copies = [pltpu.make_async_copy(refs[i], refs[count + i], sem.at[i]) for i in range(count)]
    for copy in copies:
        copy.start()
    for copy in copies:
        copy.wait()


def solution(mesh):
    n_sp, n_tp = mesh.shape["sp"], mesh.shape["tp"]

    def local(queries, keys, values, gains, bias_table, d_out):
        rows, width = queries.shape
        heads = width // HEAD_DIM
        half = rows // 2
        assert n_sp > 1 and rows == LEFT * SEG and half == MAX_REL == HEAD_DIM and 2 * heads + 1 <= 8
        act = jax.ShapeDtypeStruct((rows, width), BF16)
        vmem = pl.BlockSpec(memory_space=pltpu.VMEM)
        shapes = (
            act, act, act,
            jax.ShapeDtypeStruct(bias_table.shape[::-1], F32),
            jax.ShapeDtypeStruct(gains.shape, F32),
        )
        low = pltpu.VMEM((heads, rows, HEAD_DIM), BF16)
        pair = pltpu.VMEM((2 * heads, rows, HEAD_DIM), BF16)
        wide = pltpu.VMEM((heads, rows, HEAD_DIM), F32)
        thin = pltpu.VMEM((heads, rows, 1), F32)
        parts = pl.pallas_call(
            functools.partial(kernel, n_sp, n_tp),
            out_shape=shapes,
            in_specs=[pl.BlockSpec(memory_space=pltpu.HBM)] * 6,
            out_specs=(vmem,) * 5,
            scratch_shapes=[
                pair, pair,
                pltpu.VMEM(gains.shape, F32),
                pltpu.VMEM(bias_table.shape[::-1], F32),
                low, low,
                pltpu.VMEM((heads, 2 * rows, HEAD_DIM), BF16),
                low,
                wide, thin, wide, thin,
                pltpu.VMEM((heads, 5, half, half), F32),
                pltpu.VMEM((heads, 3, half, half), F32),
                pltpu.VMEM((heads, 3, half, half), F32),
                wide, wide,
                pair, low, low,
                pltpu.VMEM((8, HEAD_DIM), F32),
                pltpu.VMEM((n_sp, 8, HEAD_DIM), F32),
                pltpu.VMEM((1, HEAD_DIM), F32),
                pltpu.VMEM((n_tp - 1, n_sp, 1, HEAD_DIM), F32),
                pltpu.SemaphoreType.DMA((4,)),
                pltpu.SemaphoreType.DMA((4 * heads,)),
                pltpu.SemaphoreType.DMA((2,)),
                pltpu.SemaphoreType.REGULAR((max(1, (n_sp - 1).bit_length()),)),
            ],
            compiler_params=pltpu.CompilerParams(
                collective_id=0, has_side_effects=True, vmem_limit_bytes=24 * 1024 * 1024
            ),
        )(*(
            pltpu.with_memory_space_constraint(x, pltpu.HBM)
            for x in (queries, keys, values, d_out, gains, bias_table.T)
        ))
        d_q, d_k, d_v, d_table, d_gains = pl.pallas_call(
            emit,
            out_shape=shapes,
            in_specs=[vmem] * 5,
            out_specs=(pl.BlockSpec(memory_space=pltpu.HBM),) * 5,
            scratch_shapes=[pltpu.SemaphoreType.DMA((5,))],
            compiler_params=pltpu.CompilerParams(vmem_limit_bytes=8 * 1024 * 1024),
        )(*parts)
        return d_q, d_k, d_v, d_table.T, d_gains

    in_specs = (P("sp", "tp"), P("sp", "tp"), P("sp", "tp"), P(), P(None, "tp"), P("sp", "tp"))
    out_specs = (P("sp", "tp"), P("sp", "tp"), P("sp", "tp"), P(None, "tp"), P())
    return jax.shard_map(local, mesh=mesh, in_specs=in_specs, out_specs=out_specs, check_vma=False)
```

```python
import functools

import jax
import jax.numpy as jnp
from jax import lax
from jax.experimental import pallas as pl
from jax.experimental.pallas import tpu as pltpu
from jax.sharding import PartitionSpec as P

HEAD_DIM = 128
SEG = 64
LEFT = 4
MAX_REL = 128
EPSILON = 1e-06
NEG = -1e30
LOG2E = 1.4426950408889634
MESH = pl.DeviceIdType.MESH
F32 = jnp.float32
BF16 = jnp.bfloat16


def dot(a, b, contract):
    return lax.dot_general(a, b, ((contract[:1], contract[1:]), ((), ())), preferred_element_type=F32)


def unit_of(block):
    wide = block.astype(F32)
    rms = lax.rsqrt(jnp.mean(wide * wide, axis=-1, keepdims=True) + EPSILON)
    return wide * rms, rms


def fold(tile, lead):
    total = None
    for start in range(0, tile.shape[0], 8):
        turned = pltpu.roll(tile[start : start + 8], (lead - start) % tile.shape[1], 1)
        total = turned if total is None else total + turned
    return total


def align(total):
    lanes = total.shape[1]
    sublane = lax.broadcasted_iota(jnp.int32, total.shape, 0)
    line = jnp.where(sublane == 0, total, 0.0)
    for i in range(1, 8):
        line = line + jnp.where(sublane == i, pltpu.roll(total, lanes - i, 1), 0.0)
    return jnp.sum(line, axis=0, keepdims=True)


def kernel(
    n_sp, n_tp,
    q_hbm, k_hbm, v_hbm, do_hbm, g_hbm, t_hbm,
    dq_ref, dk_ref, dv_ref, dt_ref, dg_ref,
    kv_ref, qd_ref, g_ref, t_ref, k_raw, v_prev, kn, qn, q_unit, q_rms, k_unit, k_rms,
    tiles, e_own, dp_own, dk_acc, dv_acc, out_ref, dk_in, dv_in, one_src, two, line_src, lines,
    load_sem, recv_sem, red_sem, hand_sem,
):
    heads, rows, _ = k_raw.shape
    k_ref, v_ref = kv_ref.at[pl.ds(0, heads)], kv_ref.at[pl.ds(heads, heads)]
    q_ref, do_ref = qd_ref.at[pl.ds(0, heads)], qd_ref.at[pl.ds(heads, heads)]
    dk_out, dv_out = out_ref.at[pl.ds(0, heads)], out_ref.at[pl.ds(heads, heads)]
    half = rows // 2
    entries = t_ref.shape[1]
    lead = SEG - 1
    factor = HEAD_DIM ** (-0.5)
    scale = factor * LOG2E
    sp, tp = lax.axis_index("sp"), lax.axis_index("tp")
    has_prev, has_next = sp > 0, sp < n_sp - 1
    nxt, prv = sp + 1, sp - 1

    def load(src, dst, slot):
        return pltpu.make_async_copy(src, dst, load_sem.at[slot])

    def by_head(src, dst, slot):
        return [load(src.at[:, pl.ds(h * HEAD_DIM, HEAD_DIM)], dst.at[h], slot) for h in range(heads)]

    def drain(ref, sem):
        pltpu.make_async_copy(ref, ref, sem).wait()

    def signal(sem, at, core):
        pl.semaphore_signal(sem, inc=1, device_id=(at, core), device_id_type=MESH)

    def around(sem, radius):
        @pl.when(sp >= radius)
        def _():
            signal(sem, sp - radius, tp)

        @pl.when(sp < n_sp - radius)
        def _():
            signal(sem, sp + radius, tp)

    def count_around(radius):
        return jnp.where(sp >= radius, 1, 0) + jnp.where(sp < n_sp - radius, 1, 0)

    barrier = pltpu.get_barrier_semaphore()
    around(barrier, 1)
    for other in range(1, n_tp):
        signal(barrier, sp, lax.rem(tp + other, n_tp))
    load_small = [load(t_hbm, t_ref, 2), load(g_hbm, g_ref, 3)]
    for copy in (
        by_head(k_hbm, k_ref, 0) + by_head(v_hbm, v_ref, 0) + load_small
        + by_head(q_hbm, q_ref, 1) + by_head(do_hbm, do_ref, 1)
    ):
        copy.start()

    pl.semaphore_wait(barrier, count_around(1) + n_tp - 1)

    rounds = []
    while 2 ** len(rounds) < n_sp:
        rounds.append(2 ** len(rounds))

    def say(step):
        around(hand_sem.at[step], rounds[step])

    def hear(step):
        pl.semaphore_wait(hand_sem.at[step], count_around(rounds[step]))

    def send(slot, src, dst, to):
        return pltpu.make_async_remote_copy(
            src_ref=src, dst_ref=dst, send_sem=load_sem.at[slot % 4 // 2], recv_sem=recv_sem.at[slot],
            device_id=(to, tp), device_id_type=MESH,
        )

    k_next = [send(4 * h, k_ref.at[h], k_raw.at[h], nxt) for h in range(heads)]
    v_next = [send(4 * h + 1, v_ref.at[h], v_prev.at[h], nxt) for h in range(heads)]
    dv_back = [send(4 * h + 2, dv_out.at[h], dv_in.at[h], prv) for h in range(heads)]
    dk_back = [send(4 * h + 3, dk_out.at[h], dk_in.at[h], prv) for h in range(heads)]

    def start(gate, copies):
        @pl.when(gate)
        def _():
            for copy in copies:
                copy.start()

    drain(kv_ref, load_sem.at[0])
    yields = tp == n_tp - 1
    eager = sp < n_sp // 4
    start(has_next, [k_next[0], v_next[0]])
    start(has_next & jnp.logical_not(yields), k_next[1:] + v_next[1:])
    say(0)
    for copy in load_small:
        copy.wait()

    @pl.when(jnp.logical_not(has_prev))
    def _():
        kn[:, 0:rows, :] = jnp.zeros((heads, rows, HEAD_DIM), BF16)
        v_prev[...] = jnp.zeros((heads, rows, HEAD_DIM), BF16)

    g0, g1 = g_ref[0:1, :], g_ref[1:2, :]
    low, high = slice(0, half), slice(half, rows)
    row = lax.broadcasted_iota(jnp.int32, (half, half), 0)
    col = lax.broadcasted_iota(jnp.int32, (half, half), 1)
    upper = col >= row
    absent = jnp.where(has_prev, 0.0, NEG)

    table = jnp.concatenate([t_ref[...], jnp.zeros((heads, 2 * half - entries), F32)], axis=1)
    table = pltpu.roll(table, 2 * half - lead, 1)
    for h in range(heads):
        def skew(line):
            return pltpu.roll(jnp.broadcast_to(line, (half, half)), 0, 1, stride=1, stride_axis=0)

        close = skew(table[h : h + 1, 0:half])
        ahead = skew(table[h : h + 1, half:])
        far = jnp.broadcast_to(table[h : h + 1, half : half + 1], (half, half))
        same = jnp.where(upper, close, ahead)
        same = jnp.where((row >= SEG) & (col < SEG), NEG, same)
        before = jnp.where(upper, far, close)
        distant = jnp.where((row < SEG) & (col >= SEG), NEG, far)
        top_own = jnp.max(same, axis=0, keepdims=True)
        top = jnp.maximum(top_own, jnp.max(before, axis=0, keepdims=True))
        first_top = jnp.where(has_prev, top, top_own)
        tiles[h, 0] = (same - first_top) * LOG2E
        tiles[h, 1] = (before - top) * LOG2E
        tiles[h, 2] = (same - top) * LOG2E
        tiles[h, 3] = (distant - top) * LOG2E + absent
        tiles[h, 4] = (before - top) * LOG2E + absent

    inverse = 1.0 / g_ref[...]
    for h in range(heads):
        unit, rms = unit_of(k_ref[h])
        k_unit[h] = unit
        k_rms[h] = rms
        kn[h, rows:, :] = (unit * g1).astype(BF16)
    drain(qd_ref, load_sem.at[1])

    sums = []
    for h in range(heads):
        unit, rms = unit_of(q_ref[h])
        q_unit[h] = unit
        q_rms[h] = rms
        qn[h] = (unit * g0).astype(BF16)
        s0 = dot(kn[h, rows : rows + half, :], qn[h], (1, 1)) * scale
        s1 = dot(kn[h, rows + half :, :], qn[h, high, :], (1, 1)) * scale
        e0 = jnp.exp2(s0[:, low] + tiles[h, 0])
        e1 = jnp.exp2(s0[:, high] + tiles[h, 1])
        e2 = jnp.exp2(s1 + tiles[h, 2])
        e_own[h, 0], e_own[h, 1], e_own[h, 2] = e0, e1, e2
        p0 = dot(v_ref[h, low, :], do_ref[h], (1, 1))
        dp_own[h, 0], dp_own[h, 1] = p0[:, low], p0[:, high]
        dp_own[h, 2] = dot(v_ref[h, high, :], do_ref[h, high, :], (1, 1))
        sums.append((
            jnp.sum(e0, axis=0, keepdims=True),
            jnp.sum(e1, axis=0, keepdims=True) + jnp.sum(e2, axis=0, keepdims=True),
        ))
    step = 0

    def relay(step):
        if step < len(rounds):
            hear(step)
            if step + 1 < len(rounds):
                say(step + 1)
        return step + 1

    step = relay(step)
    step = relay(step)
    packed = []
    mass = jnp.zeros((1, HEAD_DIM), F32)
    for h in range(heads):
        @pl.when(has_prev)
        def _():
            k_next[h].wait_recv()
            kn[h, 0:rows, :] = (unit_of(k_raw[h])[0] * g1).astype(BF16)

        s0 = dot(kn[h, low, :], qn[h, low, :], (1, 1)) * scale
        s1 = dot(kn[h, high, :], qn[h], (1, 1)) * scale
        x0 = jnp.exp2(s0 + tiles[h, 3])
        x1 = jnp.exp2(s1[:, low] + tiles[h, 4])
        x2 = jnp.exp2(s1[:, high] + tiles[h, 3])
        r0 = 1.0 / (sums[h][0] + jnp.sum(x0 + x1, axis=0, keepdims=True))
        r1 = 1.0 / (sums[h][1] + jnp.sum(x2, axis=0, keepdims=True))
        x0, x1, x2 = x0 * r0, x1 * r0, x2 * r1
        e0, e1, e2 = e_own[h, 0] * r0, e_own[h, 1] * r1, e_own[h, 2] * r1
        d_o = do_ref[h]
        dv_out[h, low, :] = dot(x0.astype(BF16), d_o[low], (1, 0)).astype(BF16)
        dv_out[h, high, :] = dot(jnp.concatenate([x1, x2], axis=1).astype(BF16), d_o, (1, 0)).astype(BF16)
        dv_acc[h, low, :] = dot(jnp.concatenate([e0, e1], axis=1).astype(BF16), d_o, (1, 0))
        dv_acc[h, high, :] = dot(e2.astype(BF16), d_o[high], (1, 0))
        if h == heads - 1:
            start(has_prev & jnp.logical_not(yields), [dv_back[h]])
        if step < len(rounds) - 1:
            step = relay(step)
        own0 = jnp.sum(e0 * dp_own[h, 0], axis=0, keepdims=True)
        own1 = jnp.sum(e1 * dp_own[h, 1] + e2 * dp_own[h, 2], axis=0, keepdims=True)

        @pl.when(has_prev)
        def _():
            v_next[h].wait_recv()

        if h == 0:
            start(has_next & yields, k_next[1:] + v_next[1:])
        p0 = dot(v_prev[h, low, :], d_o[low], (1, 1))
        p1 = dot(v_prev[h, high, :], d_o, (1, 1))
        delta0 = own0 + jnp.sum(x0 * p0 + x1 * p1[:, low], axis=0, keepdims=True)
        delta1 = own1 + jnp.sum(x2 * p1[:, high], axis=0, keepdims=True)
        x0, x1, x2 = x0 * (p0 - delta0), x1 * (p1[:, low] - delta0), x2 * (p1[:, high] - delta1)
        e0, e1, e2 = e0 * (dp_own[h, 0] - delta0), e1 * (dp_own[h, 1] - delta1), e2 * (dp_own[h, 2] - delta1)
        blocks = [
            x0.astype(BF16),
            jnp.concatenate([x1, x2], axis=1).astype(BF16),
            jnp.concatenate([e0, e1], axis=1).astype(BF16),
            e2.astype(BF16),
        ]
        spans = [low, slice(0, rows), slice(0, rows), high]
        d_k = [dot(block, qn[h, span, :], (1, 0)) for block, span in zip(blocks, spans)]
        product = None
        for i, part in enumerate(d_k):
            term = part * kn[h, i * half : (i + 1) * half, :].astype(F32)
            product = term if product is None else product + term
        mass = mass + jnp.sum(product, axis=0, keepdims=True)
        same, before = e0 + e2, x1 + e1
        fold_p = fold(jnp.where(upper, same, before), lead)
        fold_n = fold(jnp.where(upper, 0.0, same), lead)
        line_p, line_n = align(fold_p), align(fold_n)
        lane = lax.broadcasted_iota(jnp.int32, line_p.shape, 1)
        rest = -jnp.sum(jnp.sum(fold_p + fold_n, axis=0, keepdims=True), axis=1, keepdims=True)
        packed.append(jnp.where(lane < lead, line_n, line_p))
        packed.append(jnp.where(lane < lead, line_p, jnp.where(lane == lead, rest, 0.0)))
        dk_out[h, low, :] = d_k[0].astype(BF16)
        dk_out[h, high, :] = d_k[1].astype(BF16)
        dk_acc[h, low, :] = d_k[2]
        dk_acc[h, high, :] = d_k[3]
        if h < heads - 1:
            start(has_prev, [dv_back[h], dk_back[h]])
        else:
            mass = mass * factor
            line_src[...] = mass
            one_src[...] = jnp.concatenate(
                packed + [mass, jnp.zeros((8 - 1 - len(packed), HEAD_DIM), F32)], axis=0
            )
            two[sp] = one_src[...]

            def spread(i):
                at = jnp.where(i >= sp, i + 1, i)
                pltpu.make_async_remote_copy(
                    src_ref=one_src, dst_ref=two.at[sp], send_sem=load_sem.at[2], recv_sem=red_sem.at[0],
                    device_id=(at, tp), device_id_type=MESH,
                ).start()

            def spread_line(at):
                for other in range(1, n_tp):
                    pltpu.make_async_remote_copy(
                        src_ref=line_src, dst_ref=lines.at[other - 1, sp], send_sem=load_sem.at[3],
                        recv_sem=red_sem.at[1], device_id=(at, lax.rem(tp + other, n_tp)), device_id_type=MESH,
                    ).start()

            def publish():
                for late in range(step, len(rounds)):
                    relay(late)
                if n_sp <= 32:
                    for i in range(n_sp - 1):
                        spread(i)
                        spread_line(i)
                    spread_line(n_sp - 1)
                else:
                    @pl.loop(0, n_sp - 1)
                    def _(i):
                        spread(i)

                    @pl.loop(0, n_sp)
                    def _(i):
                        spread_line(i)

            @pl.when(jnp.logical_not(eager))
            def _():
                publish()

            start(has_prev & jnp.logical_not(yields), [dk_back[h]])
        for i, part in enumerate([
            dot(jnp.concatenate([blocks[0], blocks[1][:, low], blocks[2][:, low]], axis=0), kn[h, 0 : 3 * half, :], (0, 0)),
            dot(jnp.concatenate([blocks[1][:, high], blocks[2][:, high], blocks[3]], axis=0), kn[h, half:, :], (0, 0)),
        ]):
            span = slice(i * half, (i + 1) * half)
            grad = part * factor * g0
            unit = q_unit[h, span, :]
            out = q_rms[h, span, :] * (grad - unit * jnp.mean(grad * unit, axis=-1, keepdims=True))
            dq_ref[span, h * HEAD_DIM : (h + 1) * HEAD_DIM] = out.astype(BF16)

    @pl.when(eager)
    def _():
        publish()

    held = [dk_back[heads - 1], dv_back[heads - 1]]

    def add_dv(h):
        @pl.when(has_next)
        def _():
            dv_acc[h] += dv_in[h].astype(F32)

        dv_ref[:, h * HEAD_DIM : (h + 1) * HEAD_DIM] = dv_acc[h].astype(BF16)

    def finish_dv():
        @pl.when(has_next)
        def _():
            dv_back[heads - 1].wait_recv()

        add_dv(heads - 1)

    for h in range(heads):
        across = slice(h * HEAD_DIM, (h + 1) * HEAD_DIM)

        if h == heads - 1:
            @pl.when(jnp.logical_not(yields))
            def _():
                finish_dv()

        @pl.when(has_next)
        def _():
            (dv_back if h < heads - 1 else dk_back)[h].wait_recv()

        if h < heads - 1:
            add_dv(h)

            @pl.when(has_next)
            def _():
                dk_back[h].wait_recv()

        if h == 0:
            start(has_prev & yields, held)

        @pl.when(has_next)
        def _():
            dk_acc[h] += dk_in[h].astype(F32)

        unit = k_unit[h]
        grad = dk_acc[h] * factor * g1
        out = k_rms[h] * (grad - unit * jnp.mean(grad * unit, axis=-1, keepdims=True))
        dk_ref[:, across] = out.astype(BF16)

    peers = two.at[pl.ds(0, n_sp - 1)]
    drain(peers, load_sem.at[2])
    drain(lines, load_sem.at[3])

    @pl.when(has_prev)
    def _():
        drain(out_ref, load_sem.at[1])

    @pl.when(has_next)
    def _():
        drain(kv_ref, load_sem.at[0])

    drain(peers, red_sem.at[0])
    drain(lines, red_sem.at[1])
    whole = jnp.sum(two[...], axis=0)
    for h in range(heads):
        dt_ref[h : h + 1, 0:half] = whole[2 * h : 2 * h + 1]
        dt_ref[h : h + 1, half:] = whole[2 * h + 1 : 2 * h + 2, 0 : entries - half]
    mass = whole[2 * heads : 2 * heads + 1] + jnp.sum(lines[...], axis=(0, 1))
    dg_ref[...] = mass * inverse

    @pl.when(yields)
    def _():
        finish_dv()


def emit(*refs):
    sem = refs[-1]
    count = len(refs) // 2
    copies = [pltpu.make_async_copy(refs[i], refs[count + i], sem.at[i]) for i in range(count)]
    for copy in copies:
        copy.start()
    for copy in copies:
        copy.wait()


def solution(mesh):
    n_sp, n_tp = mesh.shape["sp"], mesh.shape["tp"]

    def local(queries, keys, values, gains, bias_table, d_out):
        rows, width = queries.shape
        heads = width // HEAD_DIM
        half = rows // 2
        assert n_sp > 1 and rows == LEFT * SEG and half == MAX_REL == HEAD_DIM and 2 * heads + 1 <= 8
        act = jax.ShapeDtypeStruct((rows, width), BF16)
        vmem = pl.BlockSpec(memory_space=pltpu.VMEM)
        shapes = (
            act, act, act,
            jax.ShapeDtypeStruct(bias_table.shape[::-1], F32),
            jax.ShapeDtypeStruct(gains.shape, F32),
        )
        low = pltpu.VMEM((heads, rows, HEAD_DIM), BF16)
        pair = pltpu.VMEM((2 * heads, rows, HEAD_DIM), BF16)
        wide = pltpu.VMEM((heads, rows, HEAD_DIM), F32)
        thin = pltpu.VMEM((heads, rows, 1), F32)
        parts = pl.pallas_call(
            functools.partial(kernel, n_sp, n_tp),
            out_shape=shapes,
            in_specs=[pl.BlockSpec(memory_space=pltpu.HBM)] * 6,
            out_specs=(vmem,) * 5,
            scratch_shapes=[
                pair, pair,
                pltpu.VMEM(gains.shape, F32),
                pltpu.VMEM(bias_table.shape[::-1], F32),
                low, low,
                pltpu.VMEM((heads, 2 * rows, HEAD_DIM), BF16),
                low,
                wide, thin, wide, thin,
                pltpu.VMEM((heads, 5, half, half), F32),
                pltpu.VMEM((heads, 3, half, half), F32),
                pltpu.VMEM((heads, 3, half, half), F32),
                wide, wide,
                pair, low, low,
                pltpu.VMEM((8, HEAD_DIM), F32),
                pltpu.VMEM((n_sp, 8, HEAD_DIM), F32),
                pltpu.VMEM((1, HEAD_DIM), F32),
                pltpu.VMEM((n_tp - 1, n_sp, 1, HEAD_DIM), F32),
                pltpu.SemaphoreType.DMA((4,)),
                pltpu.SemaphoreType.DMA((4 * heads,)),
                pltpu.SemaphoreType.DMA((2,)),
                pltpu.SemaphoreType.REGULAR((max(1, (n_sp - 1).bit_length()),)),
            ],
            compiler_params=pltpu.CompilerParams(
                collective_id=0, has_side_effects=True, vmem_limit_bytes=24 * 1024 * 1024
            ),
        )(*(
            pltpu.with_memory_space_constraint(x, pltpu.HBM)
            for x in (queries, keys, values, d_out, gains, bias_table.T)
        ))
        d_q, d_k, d_v, d_table, d_gains = pl.pallas_call(
            emit,
            out_shape=shapes,
            in_specs=[vmem] * 5,
            out_specs=(pl.BlockSpec(memory_space=pltpu.HBM),) * 5,
            scratch_shapes=[pltpu.SemaphoreType.DMA((5,))],
            compiler_params=pltpu.CompilerParams(vmem_limit_bytes=8 * 1024 * 1024),
        )(*parts)
        return d_q, d_k, d_v, d_table.T, d_gains

    in_specs = (P("sp", "tp"), P("sp", "tp"), P("sp", "tp"), P(), P(None, "tp"), P("sp", "tp"))
    out_specs = (P("sp", "tp"), P("sp", "tp"), P("sp", "tp"), P(None, "tp"), P())
    return jax.shard_map(local, mesh=mesh, in_specs=in_specs, out_specs=out_specs, check_vma=False)
```

```python
import functools

import jax
import jax.numpy as jnp
from jax import lax
from jax.experimental import pallas as pl
from jax.experimental.pallas import tpu as pltpu
from jax.sharding import PartitionSpec as P

HEAD_DIM = 128
SEG = 64
LEFT = 4
MAX_REL = 128
EPSILON = 1e-06
NEG = -1e30
LOG2E = 1.4426950408889634
MESH = pl.DeviceIdType.MESH
F32 = jnp.float32
BF16 = jnp.bfloat16


def dot(a, b, contract):
    return lax.dot_general(a, b, ((contract[:1], contract[1:]), ((), ())), preferred_element_type=F32)


def unit_of(block):
    wide = block.astype(F32)
    rms = lax.rsqrt(jnp.mean(wide * wide, axis=-1, keepdims=True) + EPSILON)
    return wide * rms, rms


def fold(tile, lead):
    total = None
    for start in range(0, tile.shape[0], 8):
        turned = pltpu.roll(tile[start : start + 8], (lead - start) % tile.shape[1], 1)
        total = turned if total is None else total + turned
    return total


def align(total):
    lanes = total.shape[1]
    sublane = lax.broadcasted_iota(jnp.int32, total.shape, 0)
    line = jnp.where(sublane == 0, total, 0.0)
    for i in range(1, 8):
        line = line + jnp.where(sublane == i, pltpu.roll(total, lanes - i, 1), 0.0)
    return jnp.sum(line, axis=0, keepdims=True)


def kernel(
    n_sp, n_tp,
    q_hbm, k_hbm, v_hbm, do_hbm, g_hbm, t_hbm,
    dq_ref, dk_ref, dv_ref, dt_ref, dg_ref,
    kv_ref, qd_ref, g_ref, t_ref, k_raw, v_prev, kn, qn, q_unit, q_rms, k_unit, k_rms,
    tiles, e_own, dp_own, dk_acc, dv_acc, out_ref, dk_in, dv_in, one_src, two, line_src, lines,
    load_sem, recv_sem, red_sem, hand_sem,
):
    heads, rows, _ = k_raw.shape
    k_ref, v_ref = kv_ref.at[pl.ds(0, heads)], kv_ref.at[pl.ds(heads, heads)]
    q_ref, do_ref = qd_ref.at[pl.ds(0, heads)], qd_ref.at[pl.ds(heads, heads)]
    dk_out, dv_out = out_ref.at[pl.ds(0, heads)], out_ref.at[pl.ds(heads, heads)]
    half = rows // 2
    entries = t_ref.shape[1]
    lead = SEG - 1
    factor = HEAD_DIM ** (-0.5)
    scale = factor * LOG2E
    sp, tp = lax.axis_index("sp"), lax.axis_index("tp")
    has_prev, has_next = sp > 0, sp < n_sp - 1
    nxt, prv = sp + 1, sp - 1

    def load(src, dst, slot):
        return pltpu.make_async_copy(src, dst, load_sem.at[slot])

    def by_head(src, dst, slot):
        return [load(src.at[:, pl.ds(h * HEAD_DIM, HEAD_DIM)], dst.at[h], slot) for h in range(heads)]

    def drain(ref, sem):
        pltpu.make_async_copy(ref, ref, sem).wait()

    def signal(sem, at, core):
        pl.semaphore_signal(sem, inc=1, device_id=(at, core), device_id_type=MESH)

    def around(sem, radius):
        @pl.when(sp >= radius)
        def _():
            signal(sem, sp - radius, tp)

        @pl.when(sp < n_sp - radius)
        def _():
            signal(sem, sp + radius, tp)

    def count_around(radius):
        return jnp.where(sp >= radius, 1, 0) + jnp.where(sp < n_sp - radius, 1, 0)

    barrier = pltpu.get_barrier_semaphore()
    around(barrier, 1)
    for other in range(1, n_tp):
        signal(barrier, sp, lax.rem(tp + other, n_tp))
    load_small = [load(t_hbm, t_ref, 2), load(g_hbm, g_ref, 3)]
    for copy in (
        by_head(k_hbm, k_ref, 0) + by_head(v_hbm, v_ref, 0) + load_small
        + by_head(q_hbm, q_ref, 1) + by_head(do_hbm, do_ref, 1)
    ):
        copy.start()

    pl.semaphore_wait(barrier, count_around(1) + n_tp - 1)

    rounds = []
    while 2 ** len(rounds) < n_sp:
        rounds.append(2 ** len(rounds))

    def say(step):
        around(hand_sem.at[step], rounds[step])

    def hear(step):
        pl.semaphore_wait(hand_sem.at[step], count_around(rounds[step]))

    def send(slot, src, dst, to):
        return pltpu.make_async_remote_copy(
            src_ref=src, dst_ref=dst, send_sem=load_sem.at[slot % 4 // 2], recv_sem=recv_sem.at[slot],
            device_id=(to, tp), device_id_type=MESH,
        )

    k_next = [send(4 * h, k_ref.at[h], k_raw.at[h], nxt) for h in range(heads)]
    v_next = [send(4 * h + 1, v_ref.at[h], v_prev.at[h], nxt) for h in range(heads)]
    dv_back = [send(4 * h + 2, dv_out.at[h], dv_in.at[h], prv) for h in range(heads)]
    dk_back = [send(4 * h + 3, dk_out.at[h], dk_in.at[h], prv) for h in range(heads)]

    def start(gate, copies):
        @pl.when(gate)
        def _():
            for copy in copies:
                copy.start()

    drain(kv_ref, load_sem.at[0])
    yields = tp == n_tp - 1
    eager = sp < n_sp // 4
    start(has_next, [k_next[0], v_next[0]])
    start(has_next & jnp.logical_not(yields), k_next[1:] + v_next[1:])
    say(0)
    for copy in load_small:
        copy.wait()

    @pl.when(jnp.logical_not(has_prev))
    def _():
        kn[:, 0:rows, :] = jnp.zeros((heads, rows, HEAD_DIM), BF16)
        v_prev[...] = jnp.zeros((heads, rows, HEAD_DIM), BF16)

    g0, g1 = g_ref[0:1, :], g_ref[1:2, :]
    low, high = slice(0, half), slice(half, rows)
    row = lax.broadcasted_iota(jnp.int32, (half, half), 0)
    col = lax.broadcasted_iota(jnp.int32, (half, half), 1)
    upper = col >= row
    absent = jnp.where(has_prev, 0.0, NEG)

    table = jnp.concatenate([t_ref[...], jnp.zeros((heads, 2 * half - entries), F32)], axis=1)
    table = pltpu.roll(table, 2 * half - lead, 1)
    for h in range(heads):
        def skew(line):
            return pltpu.roll(jnp.broadcast_to(line, (half, half)), 0, 1, stride=1, stride_axis=0)

        close = skew(table[h : h + 1, 0:half])
        ahead = skew(table[h : h + 1, half:])
        far = jnp.broadcast_to(table[h : h + 1, half : half + 1], (half, half))
        same = jnp.where(upper, close, ahead)
        same = jnp.where((row >= SEG) & (col < SEG), NEG, same)
        before = jnp.where(upper, far, close)
        distant = jnp.where((row < SEG) & (col >= SEG), NEG, far)
        top_own = jnp.max(same, axis=0, keepdims=True)
        top = jnp.maximum(top_own, jnp.max(before, axis=0, keepdims=True))
        first_top = jnp.where(has_prev, top, top_own)
        tiles[h, 0] = (same - first_top) * LOG2E
        tiles[h, 1] = (before - top) * LOG2E
        tiles[h, 2] = (same - top) * LOG2E
        tiles[h, 3] = (distant - top) * LOG2E + absent
        tiles[h, 4] = (before - top) * LOG2E + absent

    inverse = 1.0 / g_ref[...]
    for h in range(heads):
        unit, rms = unit_of(k_ref[h])
        k_unit[h] = unit
        k_rms[h] = rms
        kn[h, rows:, :] = (unit * g1).astype(BF16)
    drain(qd_ref, load_sem.at[1])

    sums = []
    for h in range(heads):
        unit, rms = unit_of(q_ref[h])
        q_unit[h] = unit
        q_rms[h] = rms
        qn[h] = (unit * g0).astype(BF16)
        s0 = dot(kn[h, rows : rows + half, :], qn[h], (1, 1)) * scale
        s1 = dot(kn[h, rows + half :, :], qn[h, high, :], (1, 1)) * scale
        e0 = jnp.exp2(s0[:, low] + tiles[h, 0])
        e1 = jnp.exp2(s0[:, high] + tiles[h, 1])
        e2 = jnp.exp2(s1 + tiles[h, 2])
        e_own[h, 0], e_own[h, 1], e_own[h, 2] = e0, e1, e2
        p0 = dot(v_ref[h, low, :], do_ref[h], (1, 1))
        dp_own[h, 0], dp_own[h, 1] = p0[:, low], p0[:, high]
        dp_own[h, 2] = dot(v_ref[h, high, :], do_ref[h, high, :], (1, 1))
        sums.append((
            jnp.sum(e0, axis=0, keepdims=True),
            jnp.sum(e1, axis=0, keepdims=True) + jnp.sum(e2, axis=0, keepdims=True),
        ))
    step = 0

    def relay(step):
        if step < len(rounds):
            hear(step)
            if step + 1 < len(rounds):
                say(step + 1)
        return step + 1

    step = relay(step)
    step = relay(step)
    packed = []
    mass = jnp.zeros((1, HEAD_DIM), F32)
    for h in range(heads):
        @pl.when(has_prev)
        def _():
            k_next[h].wait_recv()
            kn[h, 0:rows, :] = (unit_of(k_raw[h])[0] * g1).astype(BF16)

        s0 = dot(kn[h, low, :], qn[h, low, :], (1, 1)) * scale
        s1 = dot(kn[h, high, :], qn[h], (1, 1)) * scale
        x0 = jnp.exp2(s0 + tiles[h, 3])
        x1 = jnp.exp2(s1[:, low] + tiles[h, 4])
        x2 = jnp.exp2(s1[:, high] + tiles[h, 3])
        r0 = 1.0 / (sums[h][0] + jnp.sum(x0 + x1, axis=0, keepdims=True))
        r1 = 1.0 / (sums[h][1] + jnp.sum(x2, axis=0, keepdims=True))
        x0, x1, x2 = x0 * r0, x1 * r0, x2 * r1
        e0, e1, e2 = e_own[h, 0] * r0, e_own[h, 1] * r1, e_own[h, 2] * r1
        d_o = do_ref[h]
        dv_out[h, low, :] = dot(x0.astype(BF16), d_o[low], (1, 0)).astype(BF16)
        dv_out[h, high, :] = dot(jnp.concatenate([x1, x2], axis=1).astype(BF16), d_o, (1, 0)).astype(BF16)
        dv_acc[h, low, :] = dot(jnp.concatenate([e0, e1], axis=1).astype(BF16), d_o, (1, 0))
        dv_acc[h, high, :] = dot(e2.astype(BF16), d_o[high], (1, 0))
        start(has_prev & jnp.logical_not(yields), [dv_back[h]])
        if step < len(rounds) - 1:
            step = relay(step)
        own0 = jnp.sum(e0 * dp_own[h, 0], axis=0, keepdims=True)
        own1 = jnp.sum(e1 * dp_own[h, 1] + e2 * dp_own[h, 2], axis=0, keepdims=True)

        @pl.when(has_prev)
        def _():
            v_next[h].wait_recv()

        if h == 0:
            start(has_next & yields, k_next[1:] + v_next[1:])
        p0 = dot(v_prev[h, low, :], d_o[low], (1, 1))
        p1 = dot(v_prev[h, high, :], d_o, (1, 1))
        delta0 = own0 + jnp.sum(x0 * p0 + x1 * p1[:, low], axis=0, keepdims=True)
        delta1 = own1 + jnp.sum(x2 * p1[:, high], axis=0, keepdims=True)
        x0, x1, x2 = x0 * (p0 - delta0), x1 * (p1[:, low] - delta0), x2 * (p1[:, high] - delta1)
        e0, e1, e2 = e0 * (dp_own[h, 0] - delta0), e1 * (dp_own[h, 1] - delta1), e2 * (dp_own[h, 2] - delta1)
        blocks = [
            x0.astype(BF16),
            jnp.concatenate([x1, x2], axis=1).astype(BF16),
            jnp.concatenate([e0, e1], axis=1).astype(BF16),
            e2.astype(BF16),
        ]
        spans = [low, slice(0, rows), slice(0, rows), high]
        d_k = [dot(block, qn[h, span, :], (1, 0)) for block, span in zip(blocks, spans)]
        product = None
        for i, part in enumerate(d_k):
            term = part * kn[h, i * half : (i + 1) * half, :].astype(F32)
            product = term if product is None else product + term
        mass = mass + jnp.sum(product, axis=0, keepdims=True)
        same, before = e0 + e2, x1 + e1
        fold_p = fold(jnp.where(upper, same, before), lead)
        fold_n = fold(jnp.where(upper, 0.0, same), lead)
        line_p, line_n = align(fold_p), align(fold_n)
        lane = lax.broadcasted_iota(jnp.int32, line_p.shape, 1)
        rest = -jnp.sum(jnp.sum(fold_p + fold_n, axis=0, keepdims=True), axis=1, keepdims=True)
        packed.append(jnp.where(lane < lead, line_n, line_p))
        packed.append(jnp.where(lane < lead, line_p, jnp.where(lane == lead, rest, 0.0)))
        dk_out[h, low, :] = d_k[0].astype(BF16)
        dk_out[h, high, :] = d_k[1].astype(BF16)
        dk_acc[h, low, :] = d_k[2]
        dk_acc[h, high, :] = d_k[3]
        if h < heads - 1:
            start(has_prev & yields, [dv_back[h]])
            start(has_prev, [dk_back[h]])
        else:
            mass = mass * factor
            line_src[...] = mass
            one_src[...] = jnp.concatenate(
                packed + [mass, jnp.zeros((8 - 1 - len(packed), HEAD_DIM), F32)], axis=0
            )
            two[sp] = one_src[...]

            def spread(i):
                at = jnp.where(i >= sp, i + 1, i)
                pltpu.make_async_remote_copy(
                    src_ref=one_src, dst_ref=two.at[sp], send_sem=load_sem.at[2], recv_sem=red_sem.at[0],
                    device_id=(at, tp), device_id_type=MESH,
                ).start()

            def spread_line(at):
                for other in range(1, n_tp):
                    pltpu.make_async_remote_copy(
                        src_ref=line_src, dst_ref=lines.at[other - 1, sp], send_sem=load_sem.at[3],
                        recv_sem=red_sem.at[1], device_id=(at, lax.rem(tp + other, n_tp)), device_id_type=MESH,
                    ).start()

            def publish():
                for late in range(step, len(rounds)):
                    relay(late)
                if n_sp <= 32:
                    for i in range(n_sp - 1):
                        spread(i)
                        spread_line(i)
                    spread_line(n_sp - 1)
                else:
                    @pl.loop(0, n_sp - 1)
                    def _(i):
                        spread(i)

                    @pl.loop(0, n_sp)
                    def _(i):
                        spread_line(i)

            @pl.when(jnp.logical_not(eager))
            def _():
                publish()

            start(has_prev & jnp.logical_not(yields), [dk_back[h]])
        for i, part in enumerate([
            dot(jnp.concatenate([blocks[0], blocks[1][:, low], blocks[2][:, low]], axis=0), kn[h, 0 : 3 * half, :], (0, 0)),
            dot(jnp.concatenate([blocks[1][:, high], blocks[2][:, high], blocks[3]], axis=0), kn[h, half:, :], (0, 0)),
        ]):
            span = slice(i * half, (i + 1) * half)
            grad = part * factor * g0
            unit = q_unit[h, span, :]
            out = q_rms[h, span, :] * (grad - unit * jnp.mean(grad * unit, axis=-1, keepdims=True))
            dq_ref[span, h * HEAD_DIM : (h + 1) * HEAD_DIM] = out.astype(BF16)

    @pl.when(eager)
    def _():
        publish()

    held = [dk_back[heads - 1], dv_back[heads - 1]]

    def add_dv(h):
        @pl.when(has_next)
        def _():
            dv_acc[h] += dv_in[h].astype(F32)

        dv_ref[:, h * HEAD_DIM : (h + 1) * HEAD_DIM] = dv_acc[h].astype(BF16)

    def finish_dv():
        @pl.when(has_next)
        def _():
            dv_back[heads - 1].wait_recv()

        add_dv(heads - 1)

    for h in range(heads):
        across = slice(h * HEAD_DIM, (h + 1) * HEAD_DIM)

        if h == heads - 1:
            @pl.when(jnp.logical_not(yields))
            def _():
                finish_dv()

        @pl.when(has_next)
        def _():
            (dv_back if h < heads - 1 else dk_back)[h].wait_recv()

        if h < heads - 1:
            add_dv(h)

            @pl.when(has_next)
            def _():
                dk_back[h].wait_recv()

        if h == 0:
            start(has_prev & yields, held)

        @pl.when(has_next)
        def _():
            dk_acc[h] += dk_in[h].astype(F32)

        unit = k_unit[h]
        grad = dk_acc[h] * factor * g1
        out = k_rms[h] * (grad - unit * jnp.mean(grad * unit, axis=-1, keepdims=True))
        dk_ref[:, across] = out.astype(BF16)

    peers = two.at[pl.ds(0, n_sp - 1)]
    drain(peers, red_sem.at[0])
    drain(lines, red_sem.at[1])
    whole = jnp.sum(two[...], axis=0)
    for h in range(heads):
        dt_ref[h : h + 1, 0:half] = whole[2 * h : 2 * h + 1]
        dt_ref[h : h + 1, half:] = whole[2 * h + 1 : 2 * h + 2, 0 : entries - half]
    mass = whole[2 * heads : 2 * heads + 1] + jnp.sum(lines[...], axis=(0, 1))
    dg_ref[...] = mass * inverse

    drain(peers, load_sem.at[2])
    drain(lines, load_sem.at[3])

    @pl.when(has_prev)
    def _():
        drain(out_ref, load_sem.at[1])

    @pl.when(has_next)
    def _():
        drain(kv_ref, load_sem.at[0])

    @pl.when(yields)
    def _():
        finish_dv()


def emit(*refs):
    sem = refs[-1]
    count = len(refs) // 2
    copies = [pltpu.make_async_copy(refs[i], refs[count + i], sem.at[i]) for i in range(count)]
    for copy in copies:
        copy.start()
    for copy in copies:
        copy.wait()


def solution(mesh):
    n_sp, n_tp = mesh.shape["sp"], mesh.shape["tp"]

    def local(queries, keys, values, gains, bias_table, d_out):
        rows, width = queries.shape
        heads = width // HEAD_DIM
        half = rows // 2
        assert n_sp > 1 and rows == LEFT * SEG and half == MAX_REL == HEAD_DIM and 2 * heads + 1 <= 8
        act = jax.ShapeDtypeStruct((rows, width), BF16)
        vmem = pl.BlockSpec(memory_space=pltpu.VMEM)
        shapes = (
            act, act, act,
            jax.ShapeDtypeStruct(bias_table.shape[::-1], F32),
            jax.ShapeDtypeStruct(gains.shape, F32),
        )
        low = pltpu.VMEM((heads, rows, HEAD_DIM), BF16)
        pair = pltpu.VMEM((2 * heads, rows, HEAD_DIM), BF16)
        wide = pltpu.VMEM((heads, rows, HEAD_DIM), F32)
        thin = pltpu.VMEM((heads, rows, 1), F32)
        parts = pl.pallas_call(
            functools.partial(kernel, n_sp, n_tp),
            out_shape=shapes,
            in_specs=[pl.BlockSpec(memory_space=pltpu.HBM)] * 6,
            out_specs=(vmem,) * 5,
            scratch_shapes=[
                pair, pair,
                pltpu.VMEM(gains.shape, F32),
                pltpu.VMEM(bias_table.shape[::-1], F32),
                low, low,
                pltpu.VMEM((heads, 2 * rows, HEAD_DIM), BF16),
                low,
                wide, thin, wide, thin,
                pltpu.VMEM((heads, 5, half, half), F32),
                pltpu.VMEM((heads, 3, half, half), F32),
                pltpu.VMEM((heads, 3, half, half), F32),
                wide, wide,
                pair, low, low,
                pltpu.VMEM((8, HEAD_DIM), F32),
                pltpu.VMEM((n_sp, 8, HEAD_DIM), F32),
                pltpu.VMEM((1, HEAD_DIM), F32),
                pltpu.VMEM((n_tp - 1, n_sp, 1, HEAD_DIM), F32),
                pltpu.SemaphoreType.DMA((4,)),
                pltpu.SemaphoreType.DMA((4 * heads,)),
                pltpu.SemaphoreType.DMA((2,)),
                pltpu.SemaphoreType.REGULAR((max(1, (n_sp - 1).bit_length()),)),
            ],
            compiler_params=pltpu.CompilerParams(
                collective_id=0, has_side_effects=True, vmem_limit_bytes=24 * 1024 * 1024
            ),
        )(*(
            pltpu.with_memory_space_constraint(x, pltpu.HBM)
            for x in (queries, keys, values, d_out, gains, bias_table.T)
        ))
        d_q, d_k, d_v, d_table, d_gains = pl.pallas_call(
            emit,
            out_shape=shapes,
            in_specs=[vmem] * 5,
            out_specs=(pl.BlockSpec(memory_space=pltpu.HBM),) * 5,
            scratch_shapes=[pltpu.SemaphoreType.DMA((5,))],
            compiler_params=pltpu.CompilerParams(vmem_limit_bytes=8 * 1024 * 1024),
        )(*parts)
        return d_q, d_k, d_v, d_table.T, d_gains

    in_specs = (P("sp", "tp"), P("sp", "tp"), P("sp", "tp"), P(), P(None, "tp"), P("sp", "tp"))
    out_specs = (P("sp", "tp"), P("sp", "tp"), P("sp", "tp"), P(None, "tp"), P())
    return jax.shard_map(local, mesh=mesh, in_specs=in_specs, out_specs=out_specs, check_vma=False)
```
